256 devices in a mesh: grp: 4 (over y, x), ep: 64 (over z, core).
Axes of the slice: x: 2, y: 2, z: 32, core: 2. Of those that a mesh axis runs over, the one named last changes fastest.
The devices are a block of a 4x8x32 slice.
Arguments:
- tokens: bfloat16 [1024, 2048], P(('grp', 'ep')), parts along dimension 0, may hold values from -6 to 6
- prior_state: float32 [1024, 32, 64, 64], P(('grp', 'ep')), parts along dimension 0, may hold values from -3 to 3
- receptance_matrix: bfloat16 [2048, 2048], P('ep'), may hold values from -0.125 to 0.125
- key_matrix: bfloat16 [2048, 2048], P('ep'), may hold values from -0.125 to 0.125
- value_matrix: bfloat16 [2048, 2048], P('ep'), may hold values from -0.125 to 0.125
- decay_lowrank_first: bfloat16 [2048, 64], replicated, may hold values from -0.125 to 0.125
- decay_lowrank_second: bfloat16 [64, 2048], replicated, may hold values from -1.5 to 1.5
- decay_channel_offset: float32 [2048], replicated, may hold values from -6 to 0
- correction_lowrank_first: bfloat16 [2048, 64], replicated, may hold values from -0.125 to 0.125
- correction_lowrank_second: bfloat16 [64, 2048], replicated, may hold values from -1.5 to 1.5
- correction_offset: float32 [2048], replicated, may hold values from -4 to 4
- gate_lowrank_first: bfloat16 [2048, 128], replicated, may hold values from -0.25 to 0.25
- gate_lowrank_second: bfloat16 [128, 2048], replicated, may hold values from -0.5 to 0.5
- key_rate_blend: float32 [2048], replicated, may hold values from 0.1 to 1.9
- self_token_scale: float32 [32, 64], replicated, may hold values from -1.2 to 1.2
- per_head_gain: float32 [2048], replicated, may hold values from 0.1 to 1.9
- per_head_bias: float32 [2048], replicated, may hold values from -1.8 to 1.8
- mixer_output_weight: bfloat16 [2048, 2048], P('ep'), may hold values from -0.125 to 0.125
- mixer_norm_gain: float32 [2048], replicated, may hold values from 0.1 to 1.9
- mixer_norm_bias: float32 [2048], replicated, may hold values from -1.8 to 1.8
- expert_norm_gain: float32 [2048], replicated, may hold values from 0.1 to 1.9
- expert_norm_bias: float32 [2048], replicated, may hold values from -1.8 to 1.8
- routes: int32 [1024, 4], P(('grp', 'ep')), parts along dimension 0, may hold values from 0 to 63, all different within a row; in each aligned block of 4 rows (0 to 3, 4 to 7, ...) at most 2 rows name the same one
- routing_weight: float32 [1024, 4], P(('grp', 'ep')), parts along dimension 0, may hold values from 0.1 to 1
- expert_gate_weight: bfloat16 [64, 2048, 512], P('ep'), may hold values from -0.125 to 0.125
- expert_up_weight: bfloat16 [64, 2048, 512], P('ep'), may hold values from -0.125 to 0.125
- expert_down_weight: bfloat16 [64, 512, 2048], P('ep'), may hold values from -0.25 to 0.25
Outputs:
- result: bfloat16 [1024, 2048], P(('grp', 'ep')), parts along dimension 0
- next_state: float32 [1024, 32, 64, 64], P(('grp', 'ep')), parts along dimension 0
The draws below stay inside these ranges and needn't reach their ends.
There are 4 independent parts, one for each index of `grp`. The reference program is written for one: setup_inputs(seed, part) draws one part's arguments, and reference() takes and returns one part's arrays. A program takes and returns all parts, laid end to end along the dimension named above; an argument that names none is the same for every part. Nothing has to cross between parts.
Inputs may be any that keep to these rules, and one draw needn't show every extreme that they name: `routes`: A row names 4 different experts. Among the rows of one device no expert is named more than 2 times, and in some device one expert is named exactly 2 times; every expert is named somewhere.
All inputs are finite; a program needn't handle non-finite values.
Results may differ from the reference program's by a relative error of at most 0.0081.
Values may be sent and summed in bfloat16 or wider, within the bound.
No kernel may reach another device: no remote copies, remote signals or barrier semaphores. Data moves between devices by JAX's collectives and lax.ppermute only.
A program may use at most 128 MiB of HBM per device.

```python
import math
import jax
import jax.numpy as jnp
import numpy as np
from jax import lax

D = 2048
MIXER_HEADS = 32
HEAD_CHANNELS = 64
W = 2048
DECAY_RANK = 64
LEARN_RANK = 64
GATE_RANK = 128
FF = 512
TOP = 4
SEQ_DEV = 4
TOKENS = 256
EXPERTS = 64
CAP = 2
N_EP = 64


def levels(own_key, extent, cuts, smallest, largest):
    factor_of, own = 1.0, jax.random.fold_in(own_key, 6)
    for axis_at, shards_of in cuts:
        heights = jnp.exp(jax.random.uniform(jax.random.fold_in(own, axis_at), (shards_of,), jnp.float32, smallest / len(cuts), largest / len(cuts)))
        factor_of = factor_of * jnp.repeat(heights, extent[axis_at] // shards_of).reshape([-1 if axis == axis_at else 1 for axis in range(len(extent))])
    return factor_of


def assign_block(rng, own, number, rows, number_of, top, reach, slope):
    order = jax.random.permutation(rng, number_of)
    heavy_load, usual = shares(number_of, rows * top, reach, slope, True), shares(number_of, rows * top, reach, slope, False)
    places = jnp.arange(number_of)

    def named(lengths, turn):
        used = int((lengths > 0).sum())
        fixed = max(1, used // 4)
        moved = fixed + (places - fixed + turn * (used - fixed)) % max(1, number_of - fixed)
        return jnp.zeros((number_of,), jnp.int32).at[order[jnp.where(places < fixed, places, moved)]].set(jnp.asarray(lengths, jnp.int32))

    lengths = jnp.where(number % 4 == 0, named(heavy_load, number // 4), named(usual, number - number // 4 - 1))
    mixed = jax.random.permutation(jax.random.fold_in(own, 3), number_of)
    source_of, receiver = mixed[0:number_of // 2 * 2:2], mixed[1:number_of // 2 * 2:2]
    room = jnp.minimum(lengths[source_of] - 1, reach - lengths[receiver]) // 2
    room = jnp.where((source_of == order[0]) | (receiver == order[0]) | (lengths[receiver] == 0), 0, jnp.maximum(room, 0))
    moved = jax.random.randint(jax.random.fold_in(own, 4), (number_of // 2,), 0, 1 << 20) % (room + 1)
    lengths = lengths.at[source_of].add(-moved).at[receiver].add(moved)
    labels = jnp.searchsorted(jnp.cumsum(lengths), jnp.arange(rows * top), side="right").astype(jnp.int32)
    listing = labels.reshape(top, rows).T
    listing = listing[jax.random.permutation(jax.random.fold_in(own, 1), rows)]
    turn = jax.random.randint(jax.random.fold_in(own, 2), (rows, 1), 0, top)
    return jnp.take_along_axis(listing, (jnp.arange(top)[None, :] + turn) % top, axis=1)


def shares(number_of, total, reach, lean, full):
    weights = [(1 << 20) // math.isqrt(standing ** lean) + 1 for standing in range(1, number_of + 1)]
    largest = reach if full else min(reach, max(-(-total // number_of), total * weights[0] // sum(weights)))
    least = 1 if total - largest >= number_of - 1 else 0
    given, spare = [largest] + [least] * (number_of - 1), total - largest - least * (number_of - 1)
    while spare > 0:
        free = [i for i in range(1, number_of) if given[i] < largest] or [i for i in range(1, number_of) if given[i] < reach]
        mass, remaining = sum([weights[i] for i in free]), spare
        for i in free:
            extra = min(reach - given[i], max(1, remaining * weights[i] // mass), spare)
            given[i] = given[i] + extra
            spare = spare - extra
    return np.array(given)


def noise(stream_key, extent, scale, limit, split=(), kind=jnp.bfloat16):
    factor_of = levels(stream_key, extent, split, -0.22, 0.18) if split else 1.0
    values = jax.random.normal(stream_key, extent, jnp.float32) * scale * factor_of
    return jnp.minimum(jnp.maximum(values, -limit), limit).astype(kind)


def setup_inputs(seed: int = 0, part: int = 0) -> dict:
    arg_keys = jax.random.split(jax.random.key(seed), 28)
    part_keys = jax.random.split(jax.random.fold_in(arg_keys[27], part), 28)
    tokens = noise(part_keys[0], (TOKENS, D), 1.0, 6.0, ((0, 64),))
    prior_state = noise(part_keys[1], (TOKENS, MIXER_HEADS, HEAD_CHANNELS, HEAD_CHANNELS), 0.3, 3.0, ((0, 64),), jnp.float32)
    receptance_matrix = noise(arg_keys[2], (D, W), D ** -0.5, 0.125, ((0, 64),))
    key_matrix = noise(arg_keys[3], (D, W), D ** -0.5, 0.125, ((0, 64),))
    value_matrix = noise(arg_keys[4], (D, W), D ** -0.5, 0.125, ((0, 64),))
    decay_lowrank_first = noise(arg_keys[5], (D, DECAY_RANK), D ** -0.5, 0.125)
    decay_lowrank_second = noise(arg_keys[6], (DECAY_RANK, W), (DECAY_RANK // 4) ** -0.5, 1.5)
    decay_channel_offset = jnp.clip(jax.random.uniform(arg_keys[7], (W,), jnp.float32, -6.0, 0.0), -6.0, 0.0)
    correction_lowrank_first = noise(arg_keys[8], (D, LEARN_RANK), D ** -0.5, 0.125)
    correction_lowrank_second = noise(arg_keys[9], (LEARN_RANK, W), (LEARN_RANK // 4) ** -0.5, 1.5)
    correction_offset = noise(arg_keys[10], (W,), 1.0, 4.0, (), jnp.float32)
    gate_lowrank_first = noise(arg_keys[11], (D, GATE_RANK), (D // 4) ** -0.5, 0.25)
    gate_lowrank_second = noise(arg_keys[12], (GATE_RANK, W), GATE_RANK ** -0.5, 0.5)
    key_rate_blend = jnp.clip(1.0 + 0.18 * jax.random.normal(arg_keys[13], (W,), jnp.float32), 0.1, 1.9)
    self_token_scale = noise(arg_keys[14], (MIXER_HEADS, HEAD_CHANNELS), 0.2, 1.2, (), jnp.float32)
    per_head_gain = jnp.clip(1.0 + 0.18 * jax.random.normal(arg_keys[15], (W,), jnp.float32), 0.1, 1.9)
    per_head_bias = noise(arg_keys[16], (W,), 0.3, 1.8, (), jnp.float32)
    mixer_output_weight = noise(arg_keys[17], (W, D), W ** -0.5, 0.125, ((0, 64),))
    mixer_norm_gain = jnp.clip(1.0 + 0.18 * jax.random.normal(arg_keys[18], (D,), jnp.float32), 0.1, 1.9)
    mixer_norm_bias = noise(arg_keys[19], (D,), 0.3, 1.8, (), jnp.float32)
    expert_norm_gain = jnp.clip(1.0 + 0.18 * jax.random.normal(arg_keys[20], (D,), jnp.float32), 0.1, 1.9)
    expert_norm_bias = noise(arg_keys[21], (D,), 0.3, 1.8, (), jnp.float32)
    routes_keys = jax.random.split(jax.random.fold_in(part_keys[22], 1), TOKENS // SEQ_DEV)
    routes_turns = jax.random.permutation(jax.random.fold_in(part_keys[22], 3), TOKENS // SEQ_DEV)
    routes = jax.vmap(lambda own, number: assign_block(jax.random.fold_in(part_keys[22], 2), own, number, SEQ_DEV, EXPERTS, TOP, CAP, 1))(routes_keys, routes_turns).reshape((TOKENS, TOP))
    routing_weight = jnp.clip(0.1 + 0.9 * jax.random.uniform(part_keys[23], (TOKENS, TOP), jnp.float32) ** levels(part_keys[23], (TOKENS, TOP), ((0, 64),), -0.2, 0.2), 0.1, 1.0)
    expert_gate_weight = noise(arg_keys[24], (EXPERTS, D, FF), D ** -0.5, 0.125, ((0, 64),))
    expert_up_weight = noise(arg_keys[25], (EXPERTS, D, FF), D ** -0.5, 0.125, ((0, 64),))
    expert_down_weight = noise(arg_keys[26], (EXPERTS, FF, D), FF ** -0.5, 0.25, ((0, 64),))
    return {"tokens": tokens, "prior_state": prior_state, "receptance_matrix": receptance_matrix, "key_matrix": key_matrix, "value_matrix": value_matrix, "decay_lowrank_first": decay_lowrank_first, "decay_lowrank_second": decay_lowrank_second, "decay_channel_offset": decay_channel_offset, "correction_lowrank_first": correction_lowrank_first, "correction_lowrank_second": correction_lowrank_second, "correction_offset": correction_offset, "gate_lowrank_first": gate_lowrank_first, "gate_lowrank_second": gate_lowrank_second, "key_rate_blend": key_rate_blend, "self_token_scale": self_token_scale, "per_head_gain": per_head_gain, "per_head_bias": per_head_bias, "mixer_output_weight": mixer_output_weight, "mixer_norm_gain": mixer_norm_gain, "mixer_norm_bias": mixer_norm_bias, "expert_norm_gain": expert_norm_gain, "expert_norm_bias": expert_norm_bias, "routes": routes, "routing_weight": routing_weight, "expert_gate_weight": expert_gate_weight, "expert_up_weight": expert_up_weight, "expert_down_weight": expert_down_weight}


def layer_norm(values_in, gain_vec, bias_vec):
    row_mean = lax.optimization_barrier(jnp.mean(values_in, -1, keepdims=True))
    centered = values_in - row_mean
    row_var = lax.optimization_barrier(jnp.mean(centered * centered, -1, keepdims=True))
    return centered * lax.rsqrt(row_var + 1e-05) * gain_vec + bias_vec

def recurrent_readout(tokens, prior_state, receptance_rows, key_rows, value_rows, decay_lowrank_first, decay_lowrank_second, decay_channel_offset, correction_lowrank_first, correction_lowrank_second, correction_offset, gate_lowrank_first, gate_lowrank_second, key_rate_blend, self_token_scale, per_head_gain, per_head_bias):
    row_count = tokens.shape[0]
    head_count = prior_state.shape[1]
    head_size = prior_state.shape[2]
    squash = jnp.tanh(jnp.dot(tokens, decay_lowrank_first, preferred_element_type=jnp.float32)).astype(jnp.bfloat16)
    pre_decay = decay_channel_offset + jnp.dot(squash, decay_lowrank_second, preferred_element_type=jnp.float32)
    decay_rate = jnp.exp(-jnp.exp(-jax.nn.softplus(-pre_decay) - 0.5))
    low_learn = jnp.dot(tokens, correction_lowrank_first, preferred_element_type=jnp.float32).astype(jnp.bfloat16)
    learn_rate = jax.nn.sigmoid(correction_offset + jnp.dot(low_learn, correction_lowrank_second, preferred_element_type=jnp.float32))
    opened = jax.nn.sigmoid(jnp.dot(tokens, gate_lowrank_first, preferred_element_type=jnp.float32)).astype(jnp.bfloat16)
    gating = jnp.dot(opened, gate_lowrank_second, preferred_element_type=jnp.float32)

    def by_head(flat_arr):
        return flat_arr.reshape(row_count, head_count, head_size)
    scaled = by_head(key_rows)
    unit_key = scaled * lax.rsqrt(lax.optimization_barrier(jnp.sum(scaled * scaled, -1, keepdims=True)) + 1e-06)
    written_key = by_head(key_rows * (1.0 + (learn_rate - 1.0) * key_rate_blend))
    receptance_by_head = by_head(receptance_rows)
    value_by_head = by_head(value_rows)
    removed = jnp.einsum('nhvk,nhk->nhv', prior_state, unit_key, precision=lax.Precision.HIGHEST)
    next_state = prior_state * by_head(decay_rate)[:, :, None, :] - removed[..., None] * (unit_key * by_head(learn_rate))[:, :, None, :] + value_by_head[..., None] * written_key[:, :, None, :]
    readout = jnp.einsum('nhvk,nhk->nhv', next_state, receptance_by_head, precision=lax.Precision.HIGHEST)
    head_mean = lax.optimization_barrier(jnp.mean(readout, -1, keepdims=True))
    head_dev = readout - head_mean
    head_var = lax.optimization_barrier(jnp.mean(head_dev * head_dev, -1, keepdims=True))
    normed = (head_dev * lax.rsqrt(head_var + 0.00064)).reshape(row_count, -1) * per_head_gain + per_head_bias
    self_token_term = lax.optimization_barrier(jnp.sum(receptance_by_head * written_key * self_token_scale, -1, keepdims=True)) * value_by_head
    mixer_result = ((normed + self_token_term.reshape(row_count, -1)) * gating).astype(jnp.bfloat16)
    return (mixer_result, next_state)

def reference(tokens, prior_state, receptance_matrix, key_matrix, value_matrix, decay_lowrank_first, decay_lowrank_second, decay_channel_offset, correction_lowrank_first, correction_lowrank_second, correction_offset, gate_lowrank_first, gate_lowrank_second, key_rate_blend, self_token_scale, per_head_gain, per_head_bias, mixer_output_weight, mixer_norm_gain, mixer_norm_bias, expert_norm_gain, expert_norm_bias, routes, routing_weight, expert_gate_weight, expert_up_weight, expert_down_weight):
    receptance_rows = jnp.dot(tokens, receptance_matrix, preferred_element_type=jnp.float32)
    key_rows = jnp.dot(tokens, key_matrix, preferred_element_type=jnp.float32)
    value_rows = jnp.dot(tokens, value_matrix, preferred_element_type=jnp.float32)
    mixer_result, next_state = recurrent_readout(tokens, prior_state, receptance_rows, key_rows, value_rows, decay_lowrank_first, decay_lowrank_second, decay_channel_offset, correction_lowrank_first, correction_lowrank_second, correction_offset, gate_lowrank_first, gate_lowrank_second, key_rate_blend, self_token_scale, per_head_gain, per_head_bias)
    mixed = jnp.dot(mixer_result, mixer_output_weight, preferred_element_type=jnp.float32)
    hidden = layer_norm(tokens.astype(jnp.float32) + mixed, mixer_norm_gain, mixer_norm_bias).astype(jnp.bfloat16)
    model_width = hidden.shape[1]
    flat_ids = routes.reshape(-1).astype(jnp.int32)
    slot_total = flat_ids.shape[0]
    sort_order = jnp.argsort(flat_ids, stable=True).astype(jnp.int32)
    sorted_ids = flat_ids[sort_order]
    expert_ids = jnp.arange(EXPERTS, dtype=jnp.int32)
    counts = lax.optimization_barrier(jnp.sum((flat_ids[None, :] == expert_ids[:, None]).astype(jnp.int32), 1))
    starts = jnp.cumsum(counts) - counts
    column = jnp.arange(N_EP * CAP, dtype=jnp.int32)

    def one_expert(expert_item):
        gate_mat, up_mat, down_mat, first_slot, slot_count = expert_item
        row_index = sort_order[jnp.minimum(first_slot + column, slot_total - 1)]
        live = (column < slot_count).astype(jnp.bfloat16)
        rows_in = hidden[row_index // TOP] * live[:, None]
        gate_val = jnp.dot(rows_in, gate_mat, preferred_element_type=jnp.float32)
        up_val = jnp.dot(rows_in, up_mat, preferred_element_type=jnp.float32)
        inner = (jax.nn.silu(gate_val) * up_val).astype(jnp.bfloat16)
        return jnp.dot(inner, down_mat, preferred_element_type=jnp.float32).astype(jnp.bfloat16)
    produced = lax.map(one_expert, (expert_gate_weight, expert_up_weight, expert_down_weight, starts, counts))
    position = jnp.arange(slot_total, dtype=jnp.int32) - starts[sorted_ids]
    sorted_out = produced[sorted_ids, position]
    flat_out = jnp.zeros_like(sorted_out).at[sort_order].set(sorted_out)
    share = routing_weight / lax.optimization_barrier(jnp.sum(routing_weight, -1, keepdims=True))
    combined = lax.optimization_barrier(jnp.sum(flat_out.reshape(-1, TOP, model_width).astype(jnp.float32) * share[..., None], 1))
    result = layer_norm(hidden.astype(jnp.float32) + combined, expert_norm_gain, expert_norm_bias).astype(jnp.bfloat16)
    return (result, next_state)
```

```python
import jax
import jax.numpy as jnp
from jax import lax
from jax.sharding import PartitionSpec as P


NEAR = 8


def near_and_far(axis):
    devices = lax.axis_size(axis)
    blocks = devices // NEAR
    near = [[NEAR * b + j for j in range(NEAR)] for b in range(blocks)]
    far = [[NEAR * b + j for b in range(blocks)] for j in range(NEAR)]
    return near, far


def swap_features(value, axis, far):
    return lax.all_to_all(value, axis, split_axis=1, concat_axis=0, tiled=True, axis_index_groups=far)


def added_on_arrival(parts, axis, groups):
    got = lax.all_to_all(parts, axis, split_axis=0, concat_axis=0, tiled=True, axis_index_groups=groups)
    return jnp.sum(got.astype(jnp.float32), axis=0)


def spread_product(rows, weight, axis, far):
    own_rows = rows.shape[0]
    swapped = swap_features(rows, axis, far)
    part = jnp.dot(swapped, weight, preferred_element_type=jnp.float32).astype(jnp.bfloat16)
    return added_on_arrival(part.reshape(-1, own_rows, weight.shape[1]), axis, far)


def layer_norm(values_in, gain_vec, bias_vec):
    row_mean = jnp.mean(values_in, -1, keepdims=True)
    centered = values_in - row_mean
    row_var = jnp.mean(centered * centered, -1, keepdims=True)
    return centered * lax.rsqrt(row_var + 1e-05) * gain_vec + bias_vec


def recurrent_readout(
    tokens,
    prior_state,
    receptance_rows,
    key_rows,
    value_rows,
    decay_lowrank_first,
    decay_lowrank_second,
    decay_channel_offset,
    correction_lowrank_first,
    correction_lowrank_second,
    correction_offset,
    gate_lowrank_first,
    gate_lowrank_second,
    key_rate_blend,
    self_token_scale,
    per_head_gain,
    per_head_bias,
):
    row_count = tokens.shape[0]
    head_count = prior_state.shape[1]
    head_size = prior_state.shape[2]
    squash = jnp.tanh(
        jnp.dot(tokens, decay_lowrank_first, preferred_element_type=jnp.float32)
    ).astype(jnp.bfloat16)
    pre_decay = decay_channel_offset + jnp.dot(
        squash, decay_lowrank_second, preferred_element_type=jnp.float32
    )
    decay_rate = jnp.exp(-jnp.exp(-jax.nn.softplus(-pre_decay) - 0.5))
    low_learn = jnp.dot(
        tokens, correction_lowrank_first, preferred_element_type=jnp.float32
    ).astype(jnp.bfloat16)
    learn_rate = jax.nn.sigmoid(
        correction_offset
        + jnp.dot(low_learn, correction_lowrank_second, preferred_element_type=jnp.float32)
    )
    opened = jax.nn.sigmoid(
        jnp.dot(tokens, gate_lowrank_first, preferred_element_type=jnp.float32)
    ).astype(jnp.bfloat16)
    gating = jnp.dot(opened, gate_lowrank_second, preferred_element_type=jnp.float32)

    def by_head(flat_arr):
        return flat_arr.reshape(row_count, head_count, head_size)

    scaled = by_head(key_rows)
    unit_key = scaled * lax.rsqrt(jnp.sum(scaled * scaled, -1, keepdims=True) + 1e-06)
    written_key = by_head(key_rows * (1.0 + (learn_rate - 1.0) * key_rate_blend))
    receptance_by_head = by_head(receptance_rows)
    value_by_head = by_head(value_rows)
    removed = jnp.einsum("nhvk,nhk->nhv", prior_state, unit_key, precision=lax.Precision.HIGHEST)
    next_state = (
        prior_state * by_head(decay_rate)[:, :, None, :]
        - removed[..., None] * (unit_key * by_head(learn_rate))[:, :, None, :]
        + value_by_head[..., None] * written_key[:, :, None, :]
    )
    readout = jnp.einsum(
        "nhvk,nhk->nhv", next_state, receptance_by_head, precision=lax.Precision.HIGHEST
    )
    head_mean = jnp.mean(readout, -1, keepdims=True)
    head_dev = readout - head_mean
    head_var = jnp.mean(head_dev * head_dev, -1, keepdims=True)
    normed = (head_dev * lax.rsqrt(head_var + 0.00064)).reshape(
        row_count, -1
    ) * per_head_gain + per_head_bias
    self_token_term = (
        jnp.sum(receptance_by_head * written_key * self_token_scale, -1, keepdims=True)
        * value_by_head
    )
    mixer_result = ((normed + self_token_term.reshape(row_count, -1)) * gating).astype(jnp.bfloat16)
    return (mixer_result, next_state)


def body(
    tokens,
    prior_state,
    receptance_matrix,
    key_matrix,
    value_matrix,
    decay_lowrank_first,
    decay_lowrank_second,
    decay_channel_offset,
    correction_lowrank_first,
    correction_lowrank_second,
    correction_offset,
    gate_lowrank_first,
    gate_lowrank_second,
    key_rate_blend,
    self_token_scale,
    per_head_gain,
    per_head_bias,
    mixer_output_weight,
    mixer_norm_gain,
    mixer_norm_bias,
    expert_norm_gain,
    expert_norm_bias,
    routes,
    routing_weight,
    expert_gate_weight,
    expert_up_weight,
    expert_down_weight,
):
    own_rows, model_width = tokens.shape
    top_count = routes.shape[1]
    near, far = near_and_far("ep")
    mixer_weight = lax.all_gather(
        jnp.concatenate((receptance_matrix, key_matrix, value_matrix), axis=1),
        "ep", axis=0, tiled=True, axis_index_groups=near,
    )
    output_weight = lax.all_gather(mixer_output_weight, "ep", axis=0, tiled=True, axis_index_groups=near)
    receptance_rows, key_rows, value_rows = jnp.split(
        spread_product(tokens, mixer_weight, "ep", far), 3, axis=1
    )
    mixer_result, next_state = recurrent_readout(
        tokens,
        prior_state,
        receptance_rows,
        key_rows,
        value_rows,
        decay_lowrank_first,
        decay_lowrank_second,
        decay_channel_offset,
        correction_lowrank_first,
        correction_lowrank_second,
        correction_offset,
        gate_lowrank_first,
        gate_lowrank_second,
        key_rate_blend,
        self_token_scale,
        per_head_gain,
        per_head_bias,
    )
    mixed = spread_product(mixer_result, output_weight, "ep", far)
    hidden = layer_norm(
        tokens.astype(jnp.float32) + mixed, mixer_norm_gain, mixer_norm_bias
    ).astype(jnp.bfloat16)
    share = routing_weight / jnp.sum(routing_weight, -1, keepdims=True)
    share_high = lax.reduce_precision(share, 8, 7)
    share_low = share - share_high
    tail = jnp.concatenate((routes.astype(jnp.float32), share_high, share_low), axis=1)
    tail = jnp.pad(tail.astype(jnp.bfloat16), ((0, 0), (0, 128 - tail.shape[1])))
    gathered = lax.all_gather(
        jnp.concatenate((hidden, tail), axis=1), "ep", axis=0, tiled=True
    )
    rows_in = gathered[:, :model_width]
    tail_in = gathered[:, model_width:].astype(jnp.float32)
    named = tail_in[:, :top_count] == lax.axis_index("ep").astype(jnp.float32)
    shares = tail_in[:, top_count : 2 * top_count] + tail_in[:, 2 * top_count : 3 * top_count]
    weight_of = jnp.sum(jnp.where(named, shares, 0.0), axis=1, keepdims=True)
    gate_val = jnp.dot(rows_in, expert_gate_weight[0], preferred_element_type=jnp.float32)
    up_val = jnp.dot(rows_in, expert_up_weight[0], preferred_element_type=jnp.float32)
    inner = (jax.nn.silu(gate_val) * up_val).astype(jnp.bfloat16)
    produced = jnp.dot(inner, expert_down_weight[0], preferred_element_type=jnp.float32)
    given = (produced * weight_of).astype(jnp.bfloat16)
    by_class = given.reshape(-1, NEAR, own_rows, model_width).swapaxes(0, 1)
    block_sum = added_on_arrival(by_class, "ep", near).astype(jnp.bfloat16)
    combined = added_on_arrival(block_sum, "ep", far)
    result = layer_norm(
        hidden.astype(jnp.float32) + combined, expert_norm_gain, expert_norm_bias
    ).astype(jnp.bfloat16)
    return (result, next_state)


def solution(mesh):
    in_specs = (
        P(("grp", "ep"), None),
        P(("grp", "ep"), None, None, None),
        P("ep", None),
        P("ep", None),
        P("ep", None),
        P(),
        P(),
        P(),
        P(),
        P(),
        P(),
        P(),
        P(),
        P(),
        P(),
        P(),
        P(),
        P("ep", None),
        P(),
        P(),
        P(),
        P(),
        P(("grp", "ep"), None),
        P(("grp", "ep"), None),
        P("ep", None, None),
        P("ep", None, None),
        P("ep", None, None),
    )
    out_specs = (P(("grp", "ep"), None), P(("grp", "ep"), None, None, None))
    return jax.shard_map(body, mesh=mesh, in_specs=in_specs, out_specs=out_specs, check_vma=False)
```

```python
import jax
import jax.numpy as jnp
from jax import lax
from jax.sharding import PartitionSpec as P


NEAR = 8


def near_and_far(axis):
    devices = lax.axis_size(axis)
    blocks = devices // NEAR
    near = [[NEAR * b + j for j in range(NEAR)] for b in range(blocks)]
    far = [[NEAR * b + j for b in range(blocks)] for j in range(NEAR)]
    return near, far


def added_on_arrival(parts, axis, groups):
    got = lax.all_to_all(parts, axis, split_axis=0, concat_axis=0, tiled=True, axis_index_groups=groups)
    return jnp.sum(got.astype(jnp.float32), axis=0)


def slots_of(named, own_rows, capacity):
    owners = named.shape[0] // own_rows
    marks = named.reshape(owners, own_rows, -1).astype(jnp.float32)
    earlier = jnp.einsum("pr,orn->opn", jnp.tri(own_rows, k=-1, dtype=jnp.float32), marks)
    place = jnp.arange(owners, dtype=jnp.float32)[:, None, None] * capacity + earlier
    place = jnp.where(marks > 0, place, -1.0).reshape(owners * own_rows, -1)
    slots = jnp.arange(owners * capacity, dtype=jnp.float32)
    return place.T[:, None, :] == slots[None, :, None]


def layer_norm(values_in, gain_vec, bias_vec):
    row_mean = jnp.mean(values_in, -1, keepdims=True)
    centered = values_in - row_mean
    row_var = jnp.mean(centered * centered, -1, keepdims=True)
    return centered * lax.rsqrt(row_var + 1e-05) * gain_vec + bias_vec


def recurrent_readout(
    tokens,
    prior_state,
    receptance_rows,
    key_rows,
    value_rows,
    decay_lowrank_first,
    decay_lowrank_second,
    decay_channel_offset,
    correction_lowrank_first,
    correction_lowrank_second,
    correction_offset,
    gate_lowrank_first,
    gate_lowrank_second,
    key_rate_blend,
    self_token_scale,
    per_head_gain,
    per_head_bias,
):
    row_count = tokens.shape[0]
    head_count = prior_state.shape[1]
    head_size = prior_state.shape[2]
    squash = jnp.tanh(
        jnp.dot(tokens, decay_lowrank_first, preferred_element_type=jnp.float32)
    ).astype(jnp.bfloat16)
    pre_decay = decay_channel_offset + jnp.dot(
        squash, decay_lowrank_second, preferred_element_type=jnp.float32
    )
    decay_rate = jnp.exp(-jnp.exp(-jax.nn.softplus(-pre_decay) - 0.5))
    low_learn = jnp.dot(
        tokens, correction_lowrank_first, preferred_element_type=jnp.float32
    ).astype(jnp.bfloat16)
    learn_rate = jax.nn.sigmoid(
        correction_offset
        + jnp.dot(low_learn, correction_lowrank_second, preferred_element_type=jnp.float32)
    )
    opened = jax.nn.sigmoid(
        jnp.dot(tokens, gate_lowrank_first, preferred_element_type=jnp.float32)
    ).astype(jnp.bfloat16)
    gating = jnp.dot(opened, gate_lowrank_second, preferred_element_type=jnp.float32)

    def by_head(flat_arr):
        return flat_arr.reshape(row_count, head_count, head_size)

    scaled = by_head(key_rows)
    unit_key = scaled * lax.rsqrt(jnp.sum(scaled * scaled, -1, keepdims=True) + 1e-06)
    written_key = by_head(key_rows * (1.0 + (learn_rate - 1.0) * key_rate_blend))
    receptance_by_head = by_head(receptance_rows)
    value_by_head = by_head(value_rows)
    removed = jnp.einsum("nhvk,nhk->nhv", prior_state, unit_key, precision=lax.Precision.HIGHEST)
    next_state = (
        prior_state * by_head(decay_rate)[:, :, None, :]
        - removed[..., None] * (unit_key * by_head(learn_rate))[:, :, None, :]
        + value_by_head[..., None] * written_key[:, :, None, :]
    )
    readout = jnp.einsum(
        "nhvk,nhk->nhv", next_state, receptance_by_head, precision=lax.Precision.HIGHEST
    )
    head_mean = jnp.mean(readout, -1, keepdims=True)
    head_dev = readout - head_mean
    head_var = jnp.mean(head_dev * head_dev, -1, keepdims=True)
    normed = (head_dev * lax.rsqrt(head_var + 0.00064)).reshape(
        row_count, -1
    ) * per_head_gain + per_head_bias
    self_token_term = (
        jnp.sum(receptance_by_head * written_key * self_token_scale, -1, keepdims=True)
        * value_by_head
    )
    mixer_result = ((normed + self_token_term.reshape(row_count, -1)) * gating).astype(jnp.bfloat16)
    return (mixer_result, next_state)


def body(
    tokens,
    prior_state,
    receptance_matrix,
    key_matrix,
    value_matrix,
    decay_lowrank_first,
    decay_lowrank_second,
    decay_channel_offset,
    correction_lowrank_first,
    correction_lowrank_second,
    correction_offset,
    gate_lowrank_first,
    gate_lowrank_second,
    key_rate_blend,
    self_token_scale,
    per_head_gain,
    per_head_bias,
    mixer_output_weight,
    mixer_norm_gain,
    mixer_norm_bias,
    expert_norm_gain,
    expert_norm_bias,
    routes,
    routing_weight,
    expert_gate_weight,
    expert_up_weight,
    expert_down_weight,
):
    own_rows, model_width = tokens.shape
    top_count = routes.shape[1]
    near, far = near_and_far("ep")
    blocks = len(near)
    expert_count = lax.axis_size("ep")
    capacity = max(2, 2 * own_rows * top_count // expert_count)
    mixer_weight = lax.all_gather(
        jnp.concatenate((receptance_matrix, key_matrix, value_matrix), axis=1),
        "ep", axis=0, tiled=True, axis_index_groups=near,
    )
    with jax.named_scope("out_gather"):
        output_weight = lax.all_gather(mixer_output_weight, "ep", axis=0, tiled=True)
    share = routing_weight / jnp.sum(routing_weight, -1, keepdims=True)
    share_high = lax.reduce_precision(share, 8, 7)
    tail = jnp.concatenate((routes.astype(jnp.float32), share_high, share - share_high), axis=1)
    tail = jnp.pad(tail.astype(jnp.bfloat16), ((0, 0), (0, 128 - tail.shape[1])))
    sent = jnp.concatenate(
        (
            tokens.reshape(own_rows, blocks, -1),
            jnp.broadcast_to(tail[:, None, :], (own_rows, blocks, tail.shape[1])),
        ),
        axis=2,
    )
    swapped = lax.all_to_all(sent, "ep", split_axis=1, concat_axis=0, tiled=True, axis_index_groups=far)
    swapped = swapped.reshape(blocks * own_rows, -1)
    features = swapped[:, : model_width // blocks]
    tail_in = swapped[:, model_width // blocks :].astype(jnp.float32)
    part = jnp.dot(features, mixer_weight, preferred_element_type=jnp.float32).astype(jnp.bfloat16)
    with jax.named_scope("part_swap"):
        projected = added_on_arrival(part.reshape(blocks, own_rows, -1), "ep", far)
    receptance_rows, key_rows, value_rows = jnp.split(projected, 3, axis=1)
    first_expert = lax.axis_index("ep") // NEAR * NEAR
    experts = (first_expert + jnp.arange(NEAR)).astype(jnp.float32)
    hits = tail_in[:, :top_count, None] == experts[None, None, :]
    picked = slots_of(jnp.any(hits, axis=1), own_rows, capacity)
    dispatch = picked.reshape(-1, blocks * own_rows).astype(jnp.bfloat16)

    def shares_by_slot(first):
        by_expert = jnp.sum(jnp.where(hits, tail_in[:, first : first + top_count, None], 0.0), axis=1)
        spread = jnp.where(picked, by_expert.T[:, None, :], 0.0)
        return spread.reshape(-1, blocks * own_rows).astype(jnp.bfloat16)

    gather_high, gather_low = shares_by_slot(top_count), shares_by_slot(2 * top_count)
    mixer_result, next_state = recurrent_readout(
        tokens,
        prior_state,
        receptance_rows,
        key_rows,
        value_rows,
        decay_lowrank_first,
        decay_lowrank_second,
        decay_channel_offset,
        correction_lowrank_first,
        correction_lowrank_second,
        correction_offset,
        gate_lowrank_first,
        gate_lowrank_second,
        key_rate_blend,
        self_token_scale,
        per_head_gain,
        per_head_bias,
    )
    mixed = jnp.dot(mixer_result, output_weight, preferred_element_type=jnp.float32)
    hidden = layer_norm(
        tokens.astype(jnp.float32) + mixed, mixer_norm_gain, mixer_norm_bias
    ).astype(jnp.bfloat16)
    class_rows = lax.all_to_all(
        jnp.broadcast_to(hidden[None], (blocks, own_rows, model_width)),
        "ep", 0, 0, tiled=True, axis_index_groups=far,
    ).reshape(blocks * own_rows, model_width)
    outgoing = jnp.dot(dispatch, class_rows, preferred_element_type=jnp.float32).astype(jnp.bfloat16)
    arrived = lax.all_to_all(
        outgoing.reshape(NEAR, -1, model_width), "ep", 0, 0, tiled=True, axis_index_groups=near
    )
    flat_in = arrived.reshape(-1, model_width)
    gate_val = jnp.dot(flat_in, expert_gate_weight[0], preferred_element_type=jnp.float32)
    up_val = jnp.dot(flat_in, expert_up_weight[0], preferred_element_type=jnp.float32)
    inner = (jax.nn.silu(gate_val) * up_val).astype(jnp.bfloat16)
    produced = jnp.dot(inner, expert_down_weight[0], preferred_element_type=jnp.float32).astype(
        jnp.bfloat16
    )
    returned = lax.all_to_all(
        produced.reshape(NEAR, -1, model_width), "ep", 0, 0, tiled=True, axis_index_groups=near
    ).reshape(-1, model_width)
    over_slots = (((0,), (0,)), ((), ()))
    block_sum = lax.dot_general(
        gather_high, returned, over_slots, preferred_element_type=jnp.float32
    ) + lax.dot_general(gather_low, returned, over_slots, preferred_element_type=jnp.float32)
    combined = added_on_arrival(
        block_sum.astype(jnp.bfloat16).reshape(blocks, own_rows, model_width), "ep", far
    )
    result = layer_norm(
        hidden.astype(jnp.float32) + combined, expert_norm_gain, expert_norm_bias
    ).astype(jnp.bfloat16)
    return (result, next_state)


def solution(mesh):
    in_specs = (
        P(("grp", "ep"), None),
        P(("grp", "ep"), None, None, None),
        P("ep", None),
        P("ep", None),
        P("ep", None),
        P(),
        P(),
        P(),
        P(),
        P(),
        P(),
        P(),
        P(),
        P(),
        P(),
        P(),
        P(),
        P("ep", None),
        P(),
        P(),
        P(),
        P(),
        P(("grp", "ep"), None),
        P(("grp", "ep"), None),
        P("ep", None, None),
        P("ep", None, None),
        P("ep", None, None),
    )
    out_specs = (P(("grp", "ep"), None), P(("grp", "ep"), None, None, None))
    return jax.shard_map(body, mesh=mesh, in_specs=in_specs, out_specs=out_specs, check_vma=False)
```

```python
import jax
import jax.numpy as jnp
from jax import lax
from jax.sharding import PartitionSpec as P


NEAR = 8


def near_and_far(axis):
    devices = lax.axis_size(axis)
    blocks = devices // NEAR
    near = [[NEAR * b + j for j in range(NEAR)] for b in range(blocks)]
    far = [[NEAR * b + j for b in range(blocks)] for j in range(NEAR)]
    return near, far


def added_on_arrival(parts, axis, groups):
    got = lax.all_to_all(parts, axis, split_axis=0, concat_axis=0, tiled=True, axis_index_groups=groups)
    return jnp.sum(got.astype(jnp.float32), axis=0)


def slots_of(named, own_rows, capacity):
    owners = named.shape[0] // own_rows
    marks = named.reshape(owners, own_rows, -1).astype(jnp.float32)
    earlier = jnp.einsum("pr,orn->opn", jnp.tri(own_rows, k=-1, dtype=jnp.float32), marks)
    place = jnp.arange(owners, dtype=jnp.float32)[:, None, None] * capacity + earlier
    place = jnp.where(marks > 0, place, -1.0).reshape(owners * own_rows, -1)
    slots = jnp.arange(owners * capacity, dtype=jnp.float32)
    return place.T[:, None, :] == slots[None, :, None]


def layer_norm(values_in, gain_vec, bias_vec):
    row_mean = jnp.mean(values_in, -1, keepdims=True)
    centered = values_in - row_mean
    row_var = jnp.mean(centered * centered, -1, keepdims=True)
    return centered * lax.rsqrt(row_var + 1e-05) * gain_vec + bias_vec


def recurrent_readout(
    tokens,
    prior_state,
    receptance_rows,
    key_rows,
    value_rows,
    decay_lowrank_first,
    decay_lowrank_second,
    decay_channel_offset,
    correction_lowrank_first,
    correction_lowrank_second,
    correction_offset,
    gate_lowrank_first,
    gate_lowrank_second,
    key_rate_blend,
    self_token_scale,
    per_head_gain,
    per_head_bias,
):
    row_count = tokens.shape[0]
    head_count = prior_state.shape[1]
    head_size = prior_state.shape[2]
    squash = jnp.tanh(
        jnp.dot(tokens, decay_lowrank_first, preferred_element_type=jnp.float32)
    ).astype(jnp.bfloat16)
    pre_decay = decay_channel_offset + jnp.dot(
        squash, decay_lowrank_second, preferred_element_type=jnp.float32
    )
    decay_rate = jnp.exp(-jnp.exp(-jax.nn.softplus(-pre_decay) - 0.5))
    low_learn = jnp.dot(
        tokens, correction_lowrank_first, preferred_element_type=jnp.float32
    ).astype(jnp.bfloat16)
    learn_rate = jax.nn.sigmoid(
        correction_offset
        + jnp.dot(low_learn, correction_lowrank_second, preferred_element_type=jnp.float32)
    )
    opened = jax.nn.sigmoid(
        jnp.dot(tokens, gate_lowrank_first, preferred_element_type=jnp.float32)
    ).astype(jnp.bfloat16)
    gating = jnp.dot(opened, gate_lowrank_second, preferred_element_type=jnp.float32)

    def by_head(flat_arr):
        return flat_arr.reshape(row_count, head_count, head_size)

    scaled = by_head(key_rows)
    unit_key = scaled * lax.rsqrt(jnp.sum(scaled * scaled, -1, keepdims=True) + 1e-06)
    written_key = by_head(key_rows * (1.0 + (learn_rate - 1.0) * key_rate_blend))
    receptance_by_head = by_head(receptance_rows)
    value_by_head = by_head(value_rows)
    removed = jnp.einsum("nhvk,nhk->nhv", prior_state, unit_key, precision=lax.Precision.HIGHEST)
    next_state = (
        prior_state * by_head(decay_rate)[:, :, None, :]
        - removed[..., None] * (unit_key * by_head(learn_rate))[:, :, None, :]
        + value_by_head[..., None] * written_key[:, :, None, :]
    )
    readout = jnp.einsum(
        "nhvk,nhk->nhv", next_state, receptance_by_head, precision=lax.Precision.HIGHEST
    )
    head_mean = jnp.mean(readout, -1, keepdims=True)
    head_dev = readout - head_mean
    head_var = jnp.mean(head_dev * head_dev, -1, keepdims=True)
    normed = (head_dev * lax.rsqrt(head_var + 0.00064)).reshape(
        row_count, -1
    ) * per_head_gain + per_head_bias
    self_token_term = (
        jnp.sum(receptance_by_head * written_key * self_token_scale, -1, keepdims=True)
        * value_by_head
    )
    mixer_result = ((normed + self_token_term.reshape(row_count, -1)) * gating).astype(jnp.bfloat16)
    return (mixer_result, next_state)


def body(
    tokens,
    prior_state,
    receptance_matrix,
    key_matrix,
    value_matrix,
    decay_lowrank_first,
    decay_lowrank_second,
    decay_channel_offset,
    correction_lowrank_first,
    correction_lowrank_second,
    correction_offset,
    gate_lowrank_first,
    gate_lowrank_second,
    key_rate_blend,
    self_token_scale,
    per_head_gain,
    per_head_bias,
    mixer_output_weight,
    mixer_norm_gain,
    mixer_norm_bias,
    expert_norm_gain,
    expert_norm_bias,
    routes,
    routing_weight,
    expert_gate_weight,
    expert_up_weight,
    expert_down_weight,
):
    own_rows, model_width = tokens.shape
    top_count = routes.shape[1]
    near, far = near_and_far("ep")
    blocks = len(near)
    expert_count = lax.axis_size("ep")
    capacity = max(2, 2 * own_rows * top_count // expert_count)
    mixer_weight = lax.all_gather(
        jnp.concatenate((receptance_matrix, key_matrix, value_matrix), axis=1),
        "ep", axis=0, tiled=True, axis_index_groups=near,
    )
    output_weight = lax.all_gather(mixer_output_weight, "ep", axis=0, tiled=True, axis_index_groups=far)
    share = routing_weight / jnp.sum(routing_weight, -1, keepdims=True)
    share_high = lax.reduce_precision(share, 8, 7)
    tail = jnp.concatenate((routes.astype(jnp.float32), share_high, share - share_high), axis=1)
    tail = jnp.pad(tail.astype(jnp.bfloat16), ((0, 0), (0, 128 - tail.shape[1])))
    sent = jnp.concatenate(
        (
            tokens.reshape(own_rows, blocks, -1),
            jnp.broadcast_to(tail[:, None, :], (own_rows, blocks, tail.shape[1])),
        ),
        axis=2,
    )
    swapped = lax.all_to_all(sent, "ep", split_axis=1, concat_axis=0, tiled=True, axis_index_groups=far)
    swapped = swapped.reshape(blocks * own_rows, -1)
    features = swapped[:, : model_width // blocks]
    tail_in = swapped[:, model_width // blocks :].astype(jnp.float32)
    part = jnp.dot(features, mixer_weight, preferred_element_type=jnp.float32).astype(jnp.bfloat16)
    projected = added_on_arrival(part.reshape(blocks, own_rows, -1), "ep", far)
    receptance_rows, key_rows, value_rows = jnp.split(projected, 3, axis=1)
    first_expert = lax.axis_index("ep") // NEAR * NEAR
    experts = (first_expert + jnp.arange(NEAR)).astype(jnp.float32)
    hits = tail_in[:, :top_count, None] == experts[None, None, :]
    picked = slots_of(jnp.any(hits, axis=1), own_rows, capacity)
    dispatch = picked.reshape(-1, blocks * own_rows).astype(jnp.bfloat16)

    def shares_by_slot(first):
        by_expert = jnp.sum(jnp.where(hits, tail_in[:, first : first + top_count, None], 0.0), axis=1)
        spread = jnp.where(picked, by_expert.T[:, None, :], 0.0)
        return spread.reshape(-1, blocks * own_rows).astype(jnp.bfloat16)

    gather_high, gather_low = shares_by_slot(top_count), shares_by_slot(2 * top_count)
    mixer_result, next_state = recurrent_readout(
        tokens,
        prior_state,
        receptance_rows,
        key_rows,
        value_rows,
        decay_lowrank_first,
        decay_lowrank_second,
        decay_channel_offset,
        correction_lowrank_first,
        correction_lowrank_second,
        correction_offset,
        gate_lowrank_first,
        gate_lowrank_second,
        key_rate_blend,
        self_token_scale,
        per_head_gain,
        per_head_bias,
    )
    by_holder = mixer_result.reshape(own_rows, blocks, NEAR, -1).swapaxes(1, 2)
    channels = lax.all_to_all(
        by_holder.reshape(own_rows, NEAR, -1),
        "ep", split_axis=1, concat_axis=0, tiled=True, axis_index_groups=near,
    ).reshape(NEAR * own_rows, -1)
    mixed_part = jnp.dot(channels, output_weight, preferred_element_type=jnp.float32)
    mixed = added_on_arrival(
        mixed_part.astype(jnp.bfloat16).reshape(NEAR, own_rows, model_width), "ep", near
    )
    hidden = layer_norm(
        tokens.astype(jnp.float32) + mixed, mixer_norm_gain, mixer_norm_bias
    ).astype(jnp.bfloat16)
    class_rows = lax.all_to_all(
        jnp.broadcast_to(hidden[None], (blocks, own_rows, model_width)),
        "ep", 0, 0, tiled=True, axis_index_groups=far,
    ).reshape(blocks * own_rows, model_width)
    outgoing = jnp.dot(dispatch, class_rows, preferred_element_type=jnp.float32).astype(jnp.bfloat16)
    arrived = lax.all_to_all(
        outgoing.reshape(NEAR, -1, model_width), "ep", 0, 0, tiled=True, axis_index_groups=near
    )
    flat_in = arrived.reshape(-1, model_width)
    gate_val = jnp.dot(flat_in, expert_gate_weight[0], preferred_element_type=jnp.float32)
    up_val = jnp.dot(flat_in, expert_up_weight[0], preferred_element_type=jnp.float32)
    inner = (jax.nn.silu(gate_val) * up_val).astype(jnp.bfloat16)
    produced = jnp.dot(inner, expert_down_weight[0], preferred_element_type=jnp.float32).astype(
        jnp.bfloat16
    )
    returned = lax.all_to_all(
        produced.reshape(NEAR, -1, model_width), "ep", 0, 0, tiled=True, axis_index_groups=near
    ).reshape(-1, model_width)
    over_slots = (((0,), (0,)), ((), ()))
    block_sum = lax.dot_general(
        gather_high, returned, over_slots, preferred_element_type=jnp.float32
    ) + lax.dot_general(gather_low, returned, over_slots, preferred_element_type=jnp.float32)
    combined = added_on_arrival(
        block_sum.astype(jnp.bfloat16).reshape(blocks, own_rows, model_width), "ep", far
    )
    result = layer_norm(
        hidden.astype(jnp.float32) + combined, expert_norm_gain, expert_norm_bias
    ).astype(jnp.bfloat16)
    return (result, next_state)


def solution(mesh):
    in_specs = (
        P(("grp", "ep"), None),
        P(("grp", "ep"), None, None, None),
        P("ep", None),
        P("ep", None),
        P("ep", None),
        P(),
        P(),
        P(),
        P(),
        P(),
        P(),
        P(),
        P(),
        P(),
        P(),
        P(),
        P(),
        P("ep", None),
        P(),
        P(),
        P(),
        P(),
        P(("grp", "ep"), None),
        P(("grp", "ep"), None),
        P("ep", None, None),
        P("ep", None, None),
        P("ep", None, None),
    )
    out_specs = (P(("grp", "ep"), None), P(("grp", "ep"), None, None, None))
    return jax.shard_map(body, mesh=mesh, in_specs=in_specs, out_specs=out_specs, check_vma=False)
```

```python
import jax
import jax.numpy as jnp
from jax import lax
from jax.experimental import pallas as pl
from jax.sharding import PartitionSpec as P


NEAR = 8


def near_and_far(axis):
    devices = lax.axis_size(axis)
    blocks = devices // NEAR
    near = [[NEAR * b + j for j in range(NEAR)] for b in range(blocks)]
    far = [[NEAR * b + j for b in range(blocks)] for j in range(NEAR)]
    return near, far


def added_on_arrival(parts, axis, groups):
    got = lax.all_to_all(parts, axis, split_axis=0, concat_axis=0, tiled=True, axis_index_groups=groups)
    return jnp.sum(got.astype(jnp.float32), axis=0)


def slots_of(named, own_rows, capacity):
    owners = named.shape[0] // own_rows
    marks = named.reshape(owners, own_rows, -1).astype(jnp.float32)
    earlier = jnp.einsum("pr,orn->opn", jnp.tri(own_rows, k=-1, dtype=jnp.float32), marks)
    place = jnp.arange(owners, dtype=jnp.float32)[:, None, None] * capacity + earlier
    place = jnp.where(marks > 0, place, -1.0).reshape(owners * own_rows, -1)
    slots = jnp.arange(owners * capacity, dtype=jnp.float32)
    return place.T[:, None, :] == slots[None, :, None]


def layer_norm(values_in, gain_vec, bias_vec):
    row_mean = jnp.mean(values_in, -1, keepdims=True)
    centered = values_in - row_mean
    row_var = jnp.mean(centered * centered, -1, keepdims=True)
    return centered * lax.rsqrt(row_var + 1e-05) * gain_vec + bias_vec


def recurrence_step(projected_ref, decay_ref, learn_ref, gating_ref, blend_ref, own_ref, gain_ref, bias_ref,
                    state_ref, mixer_ref, next_ref):
    heads, size = decay_ref.shape[1], decay_ref.shape[2]
    receptance = projected_ref[0, 0:heads]
    key = projected_ref[0, heads : 2 * heads]
    value = projected_ref[0, 2 * heads : 3 * heads]
    decay, learn = decay_ref[0], learn_ref[0]
    unit = key * lax.rsqrt(jnp.sum(key * key, -1, keepdims=True) + 1e-06)
    written = key * (1.0 + (learn - 1.0) * blend_ref[...])
    unit_learn = unit * learn
    decayed = decay * receptance
    value_columns = value.T
    lane = lax.broadcasted_iota(jnp.int32, (size, heads), 1)
    removed_columns = jnp.zeros((size, heads), jnp.float32)
    kept_columns = jnp.zeros((size, heads), jnp.float32)
    for h in range(heads):
        at = slice(h, h + 1)
        state = state_ref[0, h]
        removed = jnp.sum(state * unit[at], -1, keepdims=True)
        kept = jnp.sum(state * decayed[at], -1, keepdims=True)
        next_ref[0, h] = (
            state * decay[at] - removed * unit_learn[at] + value_columns[:, at] * written[at]
        )
        removed_columns = jnp.where(lane == h, removed, removed_columns)
        kept_columns = jnp.where(lane == h, kept, kept_columns)
    readout = (
        kept_columns.T
        - removed_columns.T * jnp.sum(unit_learn * receptance, -1, keepdims=True)
        + value * jnp.sum(written * receptance, -1, keepdims=True)
    )
    centered = readout - jnp.mean(readout, -1, keepdims=True)
    spread = jnp.mean(centered * centered, -1, keepdims=True)
    normed = centered * lax.rsqrt(spread + 0.00064) * gain_ref[...] + bias_ref[...]
    own = jnp.sum(receptance * written * own_ref[...], -1, keepdims=True) * value
    mixer_ref[0] = ((normed + own) * gating_ref[0]).astype(jnp.bfloat16)


def recurrence(projected, decay, learn, gating, blend, own, gain, bias, state, interpret=False):
    rows, heads, size = state.shape[:3]
    by_row = pl.BlockSpec((1, heads, size), lambda t: (t, 0, 0))
    by_channel = pl.BlockSpec((heads, size), lambda t: (0, 0))
    by_state = pl.BlockSpec((1, heads, size, size), lambda t: (t, 0, 0, 0))

    def cut(flat):
        return flat.reshape(*flat.shape[:-1], -1, size)

    return pl.pallas_call(
        recurrence_step,
        grid=(rows,),
        in_specs=[pl.BlockSpec((1, 3 * heads, size), lambda t: (t, 0, 0))]
        + [by_row] * 3 + [by_channel] * 4 + [by_state],
        out_specs=[by_row, by_state],
        out_shape=[
            jax.ShapeDtypeStruct((rows, heads, size), jnp.bfloat16),
            jax.ShapeDtypeStruct(state.shape, jnp.float32),
        ],
        name="recurrence",
        interpret=interpret,
    )(cut(projected), cut(decay), cut(learn), cut(gating), cut(blend), own, cut(gain), cut(bias), state)


def channel_rates(
    tokens,
    decay_lowrank_first,
    decay_lowrank_second,
    decay_channel_offset,
    correction_lowrank_first,
    correction_lowrank_second,
    correction_offset,
    gate_lowrank_first,
    gate_lowrank_second,
):
    squash = jnp.tanh(
        jnp.dot(tokens, decay_lowrank_first, preferred_element_type=jnp.float32)
    ).astype(jnp.bfloat16)
    pre_decay = decay_channel_offset + jnp.dot(
        squash, decay_lowrank_second, preferred_element_type=jnp.float32
    )
    decay_rate = jnp.exp(-jnp.exp(-jax.nn.softplus(-pre_decay) - 0.5))
    low_learn = jnp.dot(
        tokens, correction_lowrank_first, preferred_element_type=jnp.float32
    ).astype(jnp.bfloat16)
    learn_rate = jax.nn.sigmoid(
        correction_offset
        + jnp.dot(low_learn, correction_lowrank_second, preferred_element_type=jnp.float32)
    )
    opened = jax.nn.sigmoid(
        jnp.dot(tokens, gate_lowrank_first, preferred_element_type=jnp.float32)
    ).astype(jnp.bfloat16)
    gating = jnp.dot(opened, gate_lowrank_second, preferred_element_type=jnp.float32)
    return decay_rate, learn_rate, gating


def body(
    tokens,
    prior_state,
    receptance_matrix,
    key_matrix,
    value_matrix,
    decay_lowrank_first,
    decay_lowrank_second,
    decay_channel_offset,
    correction_lowrank_first,
    correction_lowrank_second,
    correction_offset,
    gate_lowrank_first,
    gate_lowrank_second,
    key_rate_blend,
    self_token_scale,
    per_head_gain,
    per_head_bias,
    mixer_output_weight,
    mixer_norm_gain,
    mixer_norm_bias,
    expert_norm_gain,
    expert_norm_bias,
    routes,
    routing_weight,
    expert_gate_weight,
    expert_up_weight,
    expert_down_weight,
):
    own_rows, model_width = tokens.shape
    top_count = routes.shape[1]
    near, far = near_and_far("ep")
    blocks = len(near)
    expert_count = lax.axis_size("ep")
    capacity = max(2, 2 * own_rows * top_count // expert_count)
    mixer_weight = lax.all_gather(
        jnp.concatenate((receptance_matrix, key_matrix, value_matrix), axis=1),
        "ep", axis=0, tiled=True, axis_index_groups=near,
    )
    output_weight = lax.all_gather(mixer_output_weight, "ep", axis=0, tiled=True, axis_index_groups=far)
    share = routing_weight / jnp.sum(routing_weight, -1, keepdims=True)
    share_high = lax.reduce_precision(share, 8, 7)
    tail = jnp.concatenate((routes.astype(jnp.float32), share_high, share - share_high), axis=1)
    tail = jnp.pad(tail.astype(jnp.bfloat16), ((0, 0), (0, 128 - tail.shape[1])))
    sent = jnp.concatenate(
        (
            tokens.reshape(own_rows, blocks, -1),
            jnp.broadcast_to(tail[:, None, :], (own_rows, blocks, tail.shape[1])),
        ),
        axis=2,
    )
    swapped = lax.all_to_all(sent, "ep", split_axis=1, concat_axis=0, tiled=True, axis_index_groups=far)
    swapped = swapped.reshape(blocks * own_rows, -1)
    features = swapped[:, : model_width // blocks]
    tail_in = swapped[:, model_width // blocks :].astype(jnp.float32)
    part = jnp.dot(features, mixer_weight, preferred_element_type=jnp.float32).astype(jnp.bfloat16)
    projected = added_on_arrival(part.reshape(blocks, own_rows, -1), "ep", far)
    first_expert = lax.axis_index("ep") // NEAR * NEAR
    experts = (first_expert + jnp.arange(NEAR)).astype(jnp.float32)
    hits = tail_in[:, :top_count, None] == experts[None, None, :]
    picked = slots_of(jnp.any(hits, axis=1), own_rows, capacity)
    dispatch = picked.reshape(-1, blocks * own_rows).astype(jnp.bfloat16)

    def shares_by_slot(first):
        by_expert = jnp.sum(jnp.where(hits, tail_in[:, first : first + top_count, None], 0.0), axis=1)
        spread = jnp.where(picked, by_expert.T[:, None, :], 0.0)
        return spread.reshape(-1, blocks * own_rows).astype(jnp.bfloat16)

    gather_high, gather_low = shares_by_slot(top_count), shares_by_slot(2 * top_count)
    decay_rate, learn_rate, gating = channel_rates(
        tokens,
        decay_lowrank_first,
        decay_lowrank_second,
        decay_channel_offset,
        correction_lowrank_first,
        correction_lowrank_second,
        correction_offset,
        gate_lowrank_first,
        gate_lowrank_second,
    )
    mixer_result, next_state = recurrence(
        projected,
        decay_rate,
        learn_rate,
        gating,
        key_rate_blend,
        self_token_scale,
        per_head_gain,
        per_head_bias,
        prior_state,
    )
    by_holder = mixer_result.reshape(own_rows, blocks, NEAR, -1).swapaxes(1, 2)
    channels = lax.all_to_all(
        by_holder.reshape(own_rows, NEAR, -1),
        "ep", split_axis=1, concat_axis=0, tiled=True, axis_index_groups=near,
    ).reshape(NEAR * own_rows, -1)
    mixed_part = jnp.dot(channels, output_weight, preferred_element_type=jnp.float32)
    mixed = added_on_arrival(
        mixed_part.astype(jnp.bfloat16).reshape(NEAR, own_rows, model_width), "ep", near
    )
    hidden = layer_norm(
        tokens.astype(jnp.float32) + mixed, mixer_norm_gain, mixer_norm_bias
    ).astype(jnp.bfloat16)
    class_rows = lax.all_to_all(
        jnp.broadcast_to(hidden[None], (blocks, own_rows, model_width)),
        "ep", 0, 0, tiled=True, axis_index_groups=far,
    ).reshape(blocks * own_rows, model_width)
    outgoing = jnp.dot(dispatch, class_rows, preferred_element_type=jnp.float32).astype(jnp.bfloat16)
    arrived = lax.all_to_all(
        outgoing.reshape(NEAR, -1, model_width), "ep", 0, 0, tiled=True, axis_index_groups=near
    )
    flat_in = arrived.reshape(-1, model_width)
    gate_val = jnp.dot(flat_in, expert_gate_weight[0], preferred_element_type=jnp.float32)
    up_val = jnp.dot(flat_in, expert_up_weight[0], preferred_element_type=jnp.float32)
    inner = (jax.nn.silu(gate_val) * up_val).astype(jnp.bfloat16)
    produced = jnp.dot(inner, expert_down_weight[0], preferred_element_type=jnp.float32).astype(
        jnp.bfloat16
    )
    returned = lax.all_to_all(
        produced.reshape(NEAR, -1, model_width), "ep", 0, 0, tiled=True, axis_index_groups=near
    ).reshape(-1, model_width)
    over_slots = (((0,), (0,)), ((), ()))
    block_sum = lax.dot_general(
        gather_high, returned, over_slots, preferred_element_type=jnp.float32
    ) + lax.dot_general(gather_low, returned, over_slots, preferred_element_type=jnp.float32)
    combined = added_on_arrival(
        block_sum.astype(jnp.bfloat16).reshape(blocks, own_rows, model_width), "ep", far
    )
    result = layer_norm(
        hidden.astype(jnp.float32) + combined, expert_norm_gain, expert_norm_bias
    ).astype(jnp.bfloat16)
    return (result, next_state)


def solution(mesh):
    in_specs = (
        P(("grp", "ep"), None),
        P(("grp", "ep"), None, None, None),
        P("ep", None),
        P("ep", None),
        P("ep", None),
        P(),
        P(),
        P(),
        P(),
        P(),
        P(),
        P(),
        P(),
        P(),
        P(),
        P(),
        P(),
        P("ep", None),
        P(),
        P(),
        P(),
        P(),
        P(("grp", "ep"), None),
        P(("grp", "ep"), None),
        P("ep", None, None),
        P("ep", None, None),
        P("ep", None, None),
    )
    out_specs = (P(("grp", "ep"), None), P(("grp", "ep"), None, None, None))
    return jax.shard_map(body, mesh=mesh, in_specs=in_specs, out_specs=out_specs, check_vma=False)
```

```python
import jax
import jax.numpy as jnp
from jax import lax
from jax.experimental import pallas as pl
from jax.sharding import PartitionSpec as P


NEAR = 8


def near_and_far(axis):
    devices = lax.axis_size(axis)
    blocks = devices // NEAR
    near = [[NEAR * b + j for j in range(NEAR)] for b in range(blocks)]
    far = [[NEAR * b + j for b in range(blocks)] for j in range(NEAR)]
    return near, far


def added_on_arrival(parts, axis, groups):
    got = lax.all_to_all(parts, axis, split_axis=0, concat_axis=0, tiled=True, axis_index_groups=groups)
    return jnp.sum(got.astype(jnp.float32), axis=0)


def slots_of(named, own_rows, capacity):
    owners = named.shape[0] // own_rows
    marks = named.reshape(owners, own_rows, -1).astype(jnp.float32)
    earlier = jnp.einsum("pr,orn->opn", jnp.tri(own_rows, k=-1, dtype=jnp.float32), marks)
    place = jnp.arange(owners, dtype=jnp.float32)[:, None, None] * capacity + earlier
    place = jnp.where(marks > 0, place, -1.0).reshape(owners * own_rows, -1)
    slots = jnp.arange(owners * capacity, dtype=jnp.float32)
    return place.T[:, None, :] == slots[None, :, None]


def layer_norm(values_in, gain_vec, bias_vec):
    row_mean = jnp.mean(values_in, -1, keepdims=True)
    centered = values_in - row_mean
    row_var = jnp.mean(centered * centered, -1, keepdims=True)
    return centered * lax.rsqrt(row_var + 1e-05) * gain_vec + bias_vec


def recurrence_step(projected_ref, decay_ref, learn_ref, gating_ref, blend_ref, own_ref, gain_ref, bias_ref,
                    state_ref, mixer_ref, next_ref):
    heads, size = decay_ref.shape[1], decay_ref.shape[2]
    receptance = projected_ref[0, 0:heads]
    key = projected_ref[0, heads : 2 * heads]
    value = projected_ref[0, 2 * heads : 3 * heads]
    decay, learn = decay_ref[0], learn_ref[0]
    unit = key * lax.rsqrt(jnp.sum(key * key, -1, keepdims=True) + 1e-06)
    written = key * (1.0 + (learn - 1.0) * blend_ref[...])
    unit_learn = unit * learn
    decayed = decay * receptance
    value_columns = value.T
    lane = lax.broadcasted_iota(jnp.int32, (size, heads), 1)
    removed_columns = jnp.zeros((size, heads), jnp.float32)
    kept_columns = jnp.zeros((size, heads), jnp.float32)
    for h in range(heads):
        at = slice(h, h + 1)
        state = state_ref[0, h]
        removed = jnp.sum(state * unit[at], -1, keepdims=True)
        kept = jnp.sum(state * decayed[at], -1, keepdims=True)
        next_ref[0, h] = (
            state * decay[at] - removed * unit_learn[at] + value_columns[:, at] * written[at]
        )
        removed_columns = jnp.where(lane == h, removed, removed_columns)
        kept_columns = jnp.where(lane == h, kept, kept_columns)
    readout = (
        kept_columns.T
        - removed_columns.T * jnp.sum(unit_learn * receptance, -1, keepdims=True)
        + value * jnp.sum(written * receptance, -1, keepdims=True)
    )
    centered = readout - jnp.mean(readout, -1, keepdims=True)
    spread = jnp.mean(centered * centered, -1, keepdims=True)
    normed = centered * lax.rsqrt(spread + 0.00064) * gain_ref[...] + bias_ref[...]
    own = jnp.sum(receptance * written * own_ref[...], -1, keepdims=True) * value
    mixer_ref[0] = ((normed + own) * gating_ref[0]).astype(jnp.bfloat16)


def recurrence(projected, decay, learn, gating, blend, own, gain, bias, state, interpret=False):
    rows, heads, size = state.shape[:3]
    by_row = pl.BlockSpec((1, heads, size), lambda t: (t, 0, 0))
    by_channel = pl.BlockSpec((heads, size), lambda t: (0, 0))
    by_state = pl.BlockSpec((1, heads, size, size), lambda t: (t, 0, 0, 0))

    def cut(flat):
        return flat.reshape(*flat.shape[:-1], -1, size)

    return pl.pallas_call(
        recurrence_step,
        grid=(rows,),
        in_specs=[pl.BlockSpec((1, 3 * heads, size), lambda t: (t, 0, 0))]
        + [by_row] * 3 + [by_channel] * 4 + [by_state],
        out_specs=[by_row, by_state],
        out_shape=[
            jax.ShapeDtypeStruct((rows, heads, size), jnp.bfloat16),
            jax.ShapeDtypeStruct(state.shape, jnp.float32),
        ],
        name="recurrence",
        interpret=interpret,
    )(cut(projected), cut(decay), cut(learn), cut(gating), cut(blend), own, cut(gain), cut(bias), state)


def channel_rates(
    tokens,
    decay_lowrank_first,
    decay_lowrank_second,
    decay_channel_offset,
    correction_lowrank_first,
    correction_lowrank_second,
    correction_offset,
    gate_lowrank_first,
    gate_lowrank_second,
):
    squash = jnp.tanh(
        jnp.dot(tokens, decay_lowrank_first, preferred_element_type=jnp.float32)
    ).astype(jnp.bfloat16)
    pre_decay = decay_channel_offset + jnp.dot(
        squash, decay_lowrank_second, preferred_element_type=jnp.float32
    )
    decay_rate = jnp.exp(-jnp.exp(-jax.nn.softplus(-pre_decay) - 0.5))
    low_learn = jnp.dot(
        tokens, correction_lowrank_first, preferred_element_type=jnp.float32
    ).astype(jnp.bfloat16)
    learn_rate = jax.nn.sigmoid(
        correction_offset
        + jnp.dot(low_learn, correction_lowrank_second, preferred_element_type=jnp.float32)
    )
    opened = jax.nn.sigmoid(
        jnp.dot(tokens, gate_lowrank_first, preferred_element_type=jnp.float32)
    ).astype(jnp.bfloat16)
    gating = jnp.dot(opened, gate_lowrank_second, preferred_element_type=jnp.float32)
    return decay_rate, learn_rate, gating


def body(
    tokens,
    prior_state,
    receptance_matrix,
    key_matrix,
    value_matrix,
    decay_lowrank_first,
    decay_lowrank_second,
    decay_channel_offset,
    correction_lowrank_first,
    correction_lowrank_second,
    correction_offset,
    gate_lowrank_first,
    gate_lowrank_second,
    key_rate_blend,
    self_token_scale,
    per_head_gain,
    per_head_bias,
    mixer_output_weight,
    mixer_norm_gain,
    mixer_norm_bias,
    expert_norm_gain,
    expert_norm_bias,
    routes,
    routing_weight,
    expert_gate_weight,
    expert_up_weight,
    expert_down_weight,
):
    own_rows, model_width = tokens.shape
    top_count = routes.shape[1]
    near, far = near_and_far("ep")
    blocks = len(near)
    expert_count = lax.axis_size("ep")
    capacity = max(2, 2 * own_rows * top_count // expert_count)
    mixer_weight = lax.all_gather(
        jnp.concatenate((receptance_matrix, key_matrix, value_matrix), axis=1),
        "ep", axis=0, tiled=True, axis_index_groups=near,
    )
    groups = lax.axis_size("grp")
    share_rows = mixer_output_weight.shape[0] // groups
    weight_share = lax.dynamic_slice_in_dim(
        mixer_output_weight, lax.axis_index("grp") * share_rows, share_rows
    ).reshape(own_rows, 1, -1)
    share = routing_weight / jnp.sum(routing_weight, -1, keepdims=True)
    share_high = lax.reduce_precision(share, 8, 7)
    tail = jnp.concatenate((routes.astype(jnp.float32), share_high, share - share_high), axis=1)
    tail = jnp.pad(tail.astype(jnp.bfloat16), ((0, 0), (0, 128 - tail.shape[1])))
    sent = jnp.concatenate(
        (
            tokens.reshape(own_rows, blocks, -1),
            jnp.broadcast_to(tail[:, None, :], (own_rows, blocks, tail.shape[1])),
            jnp.broadcast_to(weight_share, (own_rows, blocks, weight_share.shape[2])),
        ),
        axis=2,
    )
    swapped = lax.all_to_all(sent, "ep", split_axis=1, concat_axis=0, tiled=True, axis_index_groups=far)
    swapped = swapped.reshape(blocks * own_rows, -1)
    body_width = model_width // blocks + tail.shape[1]
    output_weight = lax.all_gather(
        swapped[:, body_width:].reshape(blocks, share_rows, model_width), "grp", axis=1, tiled=True
    ).reshape(-1, model_width)
    features = swapped[:, : model_width // blocks]
    tail_in = swapped[:, model_width // blocks : body_width].astype(jnp.float32)
    part = jnp.dot(features, mixer_weight, preferred_element_type=jnp.float32).astype(jnp.bfloat16)
    projected = added_on_arrival(part.reshape(blocks, own_rows, -1), "ep", far)
    first_expert = lax.axis_index("ep") // NEAR * NEAR
    experts = (first_expert + jnp.arange(NEAR)).astype(jnp.float32)
    hits = tail_in[:, :top_count, None] == experts[None, None, :]
    picked = slots_of(jnp.any(hits, axis=1), own_rows, capacity)
    dispatch = picked.reshape(-1, blocks * own_rows).astype(jnp.bfloat16)

    def shares_by_slot(first):
        by_expert = jnp.sum(jnp.where(hits, tail_in[:, first : first + top_count, None], 0.0), axis=1)
        spread = jnp.where(picked, by_expert.T[:, None, :], 0.0)
        return spread.reshape(-1, blocks * own_rows).astype(jnp.bfloat16)

    gather_high, gather_low = shares_by_slot(top_count), shares_by_slot(2 * top_count)
    decay_rate, learn_rate, gating = channel_rates(
        tokens,
        decay_lowrank_first,
        decay_lowrank_second,
        decay_channel_offset,
        correction_lowrank_first,
        correction_lowrank_second,
        correction_offset,
        gate_lowrank_first,
        gate_lowrank_second,
    )
    mixer_result, next_state = recurrence(
        projected,
        decay_rate,
        learn_rate,
        gating,
        key_rate_blend,
        self_token_scale,
        per_head_gain,
        per_head_bias,
        prior_state,
    )
    by_holder = mixer_result.reshape(own_rows, blocks, NEAR, -1).swapaxes(1, 2)
    channels = lax.all_to_all(
        by_holder.reshape(own_rows, NEAR, -1),
        "ep", split_axis=1, concat_axis=0, tiled=True, axis_index_groups=near,
    ).reshape(NEAR * own_rows, -1)
    mixed_part = jnp.dot(channels, output_weight, preferred_element_type=jnp.float32)
    mixed = added_on_arrival(
        mixed_part.astype(jnp.bfloat16).reshape(NEAR, own_rows, model_width), "ep", near
    )
    hidden = layer_norm(
        tokens.astype(jnp.float32) + mixed, mixer_norm_gain, mixer_norm_bias
    ).astype(jnp.bfloat16)
    class_rows = lax.all_to_all(
        jnp.broadcast_to(hidden[None], (blocks, own_rows, model_width)),
        "ep", 0, 0, tiled=True, axis_index_groups=far,
    ).reshape(blocks * own_rows, model_width)
    outgoing = jnp.dot(dispatch, class_rows, preferred_element_type=jnp.float32).astype(jnp.bfloat16)
    arrived = lax.all_to_all(
        outgoing.reshape(NEAR, -1, model_width), "ep", 0, 0, tiled=True, axis_index_groups=near
    )
    flat_in = arrived.reshape(-1, model_width)
    gate_val = jnp.dot(flat_in, expert_gate_weight[0], preferred_element_type=jnp.float32)
    up_val = jnp.dot(flat_in, expert_up_weight[0], preferred_element_type=jnp.float32)
    inner = (jax.nn.silu(gate_val) * up_val).astype(jnp.bfloat16)
    produced = jnp.dot(inner, expert_down_weight[0], preferred_element_type=jnp.float32).astype(
        jnp.bfloat16
    )
    returned = lax.all_to_all(
        produced.reshape(NEAR, -1, model_width), "ep", 0, 0, tiled=True, axis_index_groups=near
    ).reshape(-1, model_width)
    over_slots = (((0,), (0,)), ((), ()))
    block_sum = lax.dot_general(
        gather_high, returned, over_slots, preferred_element_type=jnp.float32
    ) + lax.dot_general(gather_low, returned, over_slots, preferred_element_type=jnp.float32)
    combined = added_on_arrival(
        block_sum.astype(jnp.bfloat16).reshape(blocks, own_rows, model_width), "ep", far
    )
    result = layer_norm(
        hidden.astype(jnp.float32) + combined, expert_norm_gain, expert_norm_bias
    ).astype(jnp.bfloat16)
    return (result, next_state)


def solution(mesh):
    in_specs = (
        P(("grp", "ep"), None),
        P(("grp", "ep"), None, None, None),
        P("ep", None),
        P("ep", None),
        P("ep", None),
        P(),
        P(),
        P(),
        P(),
        P(),
        P(),
        P(),
        P(),
        P(),
        P(),
        P(),
        P(),
        P("ep", None),
        P(),
        P(),
        P(),
        P(),
        P(("grp", "ep"), None),
        P(("grp", "ep"), None),
        P("ep", None, None),
        P("ep", None, None),
        P("ep", None, None),
    )
    out_specs = (P(("grp", "ep"), None), P(("grp", "ep"), None, None, None))
    return jax.shard_map(body, mesh=mesh, in_specs=in_specs, out_specs=out_specs, check_vma=False)
```

```python
import jax
import jax.numpy as jnp
from jax import lax
from jax.experimental import pallas as pl
from jax.sharding import PartitionSpec as P


NEAR = 8


def near_and_far(axis):
    devices = lax.axis_size(axis)
    blocks = devices // NEAR
    near = [[NEAR * b + j for j in range(NEAR)] for b in range(blocks)]
    far = [[NEAR * b + j for b in range(blocks)] for j in range(NEAR)]
    return near, far


def added_on_arrival(parts, axis, groups):
    got = lax.all_to_all(parts, axis, split_axis=0, concat_axis=0, tiled=True, axis_index_groups=groups)
    return jnp.sum(got.astype(jnp.float32), axis=0)


def shifted(value, axis, steps):
    devices = lax.axis_size(axis)
    return lax.ppermute(value, axis, [(i, (i + NEAR * steps) % devices) for i in range(devices)])


def slots_of(named, own_rows, capacity):
    owners = named.shape[0] // own_rows
    marks = named.reshape(owners, own_rows, -1).astype(jnp.float32)
    earlier = jnp.einsum("pr,orn->opn", jnp.tri(own_rows, k=-1, dtype=jnp.float32), marks)
    place = jnp.arange(owners, dtype=jnp.float32)[:, None, None] * capacity + earlier
    place = jnp.where(marks > 0, place, -1.0).reshape(owners * own_rows, -1)
    slots = jnp.arange(owners * capacity, dtype=jnp.float32)
    return place.T[:, None, :] == slots[None, :, None]


def layer_norm(values_in, gain_vec, bias_vec):
    row_mean = jnp.mean(values_in, -1, keepdims=True)
    centered = values_in - row_mean
    row_var = jnp.mean(centered * centered, -1, keepdims=True)
    return centered * lax.rsqrt(row_var + 1e-05) * gain_vec + bias_vec


def recurrence_step(projected_ref, decay_ref, learn_ref, gating_ref, blend_ref, own_ref, gain_ref, bias_ref,
                    state_ref, mixer_ref, next_ref):
    heads, size = decay_ref.shape[1], decay_ref.shape[2]
    receptance = projected_ref[0, 0:heads]
    key = projected_ref[0, heads : 2 * heads]
    value = projected_ref[0, 2 * heads : 3 * heads]
    decay, learn = decay_ref[0], learn_ref[0]
    unit = key * lax.rsqrt(jnp.sum(key * key, -1, keepdims=True) + 1e-06)
    written = key * (1.0 + (learn - 1.0) * blend_ref[...])
    unit_learn = unit * learn
    decayed = decay * receptance
    value_columns = value.T
    lane = lax.broadcasted_iota(jnp.int32, (size, heads), 1)
    removed_columns = jnp.zeros((size, heads), jnp.float32)
    kept_columns = jnp.zeros((size, heads), jnp.float32)
    for h in range(heads):
        at = slice(h, h + 1)
        state = state_ref[0, h]
        removed = jnp.sum(state * unit[at], -1, keepdims=True)
        kept = jnp.sum(state * decayed[at], -1, keepdims=True)
        next_ref[0, h] = (
            state * decay[at] - removed * unit_learn[at] + value_columns[:, at] * written[at]
        )
        removed_columns = jnp.where(lane == h, removed, removed_columns)
        kept_columns = jnp.where(lane == h, kept, kept_columns)
    readout = (
        kept_columns.T
        - removed_columns.T * jnp.sum(unit_learn * receptance, -1, keepdims=True)
        + value * jnp.sum(written * receptance, -1, keepdims=True)
    )
    centered = readout - jnp.mean(readout, -1, keepdims=True)
    spread = jnp.mean(centered * centered, -1, keepdims=True)
    normed = centered * lax.rsqrt(spread + 0.00064) * gain_ref[...] + bias_ref[...]
    own = jnp.sum(receptance * written * own_ref[...], -1, keepdims=True) * value
    mixer_ref[0] = ((normed + own) * gating_ref[0]).astype(jnp.bfloat16)


def recurrence(projected, decay, learn, gating, blend, own, gain, bias, state, interpret=False):
    rows, heads, size = state.shape[:3]
    by_row = pl.BlockSpec((1, heads, size), lambda t: (t, 0, 0))
    by_channel = pl.BlockSpec((heads, size), lambda t: (0, 0))
    by_state = pl.BlockSpec((1, heads, size, size), lambda t: (t, 0, 0, 0))

    def cut(flat):
        return flat.reshape(*flat.shape[:-1], -1, size)

    return pl.pallas_call(
        recurrence_step,
        grid=(rows,),
        in_specs=[pl.BlockSpec((1, 3 * heads, size), lambda t: (t, 0, 0))]
        + [by_row] * 3 + [by_channel] * 4 + [by_state],
        out_specs=[by_row, by_state],
        out_shape=[
            jax.ShapeDtypeStruct((rows, heads, size), jnp.bfloat16),
            jax.ShapeDtypeStruct(state.shape, jnp.float32),
        ],
        name="recurrence",
        interpret=interpret,
    )(cut(projected), cut(decay), cut(learn), cut(gating), cut(blend), own, cut(gain), cut(bias), state)


def channel_rates(
    tokens,
    decay_lowrank_first,
    decay_lowrank_second,
    decay_channel_offset,
    correction_lowrank_first,
    correction_lowrank_second,
    correction_offset,
    gate_lowrank_first,
    gate_lowrank_second,
):
    squash = jnp.tanh(
        jnp.dot(tokens, decay_lowrank_first, preferred_element_type=jnp.float32)
    ).astype(jnp.bfloat16)
    pre_decay = decay_channel_offset + jnp.dot(
        squash, decay_lowrank_second, preferred_element_type=jnp.float32
    )
    decay_rate = jnp.exp(-jnp.exp(-jax.nn.softplus(-pre_decay) - 0.5))
    low_learn = jnp.dot(
        tokens, correction_lowrank_first, preferred_element_type=jnp.float32
    ).astype(jnp.bfloat16)
    learn_rate = jax.nn.sigmoid(
        correction_offset
        + jnp.dot(low_learn, correction_lowrank_second, preferred_element_type=jnp.float32)
    )
    opened = jax.nn.sigmoid(
        jnp.dot(tokens, gate_lowrank_first, preferred_element_type=jnp.float32)
    ).astype(jnp.bfloat16)
    gating = jnp.dot(opened, gate_lowrank_second, preferred_element_type=jnp.float32)
    return decay_rate, learn_rate, gating


def body(
    tokens,
    prior_state,
    receptance_matrix,
    key_matrix,
    value_matrix,
    decay_lowrank_first,
    decay_lowrank_second,
    decay_channel_offset,
    correction_lowrank_first,
    correction_lowrank_second,
    correction_offset,
    gate_lowrank_first,
    gate_lowrank_second,
    key_rate_blend,
    self_token_scale,
    per_head_gain,
    per_head_bias,
    mixer_output_weight,
    mixer_norm_gain,
    mixer_norm_bias,
    expert_norm_gain,
    expert_norm_bias,
    routes,
    routing_weight,
    expert_gate_weight,
    expert_up_weight,
    expert_down_weight,
):
    own_rows, model_width = tokens.shape
    top_count = routes.shape[1]
    near, far = near_and_far("ep")
    blocks = len(near)
    expert_count = lax.axis_size("ep")
    capacity = max(2, 2 * own_rows * top_count // expert_count)
    mixer_weight = lax.all_gather(
        jnp.concatenate((receptance_matrix, key_matrix, value_matrix), axis=1),
        "ep", axis=0, tiled=True, axis_index_groups=near,
    )
    groups = lax.axis_size("grp")
    share_rows = mixer_output_weight.shape[0] // groups
    weight_share = lax.dynamic_slice_in_dim(
        mixer_output_weight, lax.axis_index("grp") * share_rows, share_rows
    ).reshape(own_rows, 1, -1)
    share = routing_weight / jnp.sum(routing_weight, -1, keepdims=True)
    share_high = lax.reduce_precision(share, 8, 7)
    tail = jnp.concatenate((routes.astype(jnp.float32), share_high, share - share_high), axis=1)
    tail = jnp.pad(tail.astype(jnp.bfloat16), ((0, 0), (0, 128 - tail.shape[1])))
    sent = jnp.concatenate(
        (
            tokens.reshape(own_rows, blocks, -1),
            jnp.broadcast_to(tail[:, None, :], (own_rows, blocks, tail.shape[1])),
            jnp.broadcast_to(weight_share, (own_rows, blocks, weight_share.shape[2])),
        ),
        axis=2,
    )
    swapped = lax.all_to_all(sent, "ep", split_axis=1, concat_axis=0, tiled=True, axis_index_groups=far)
    swapped = swapped.reshape(blocks * own_rows, -1)
    body_width = model_width // blocks + tail.shape[1]
    output_weight = lax.all_gather(
        swapped[:, body_width:].reshape(blocks, share_rows, model_width), "grp", axis=1, tiled=True
    ).reshape(-1, model_width)
    features = swapped[:, : model_width // blocks]
    step = jnp.arange(blocks)
    source = (lax.axis_index("ep") // NEAR - step) % blocks
    turned = (source[:, None] == step[None, :]).astype(jnp.bfloat16)
    tail_in = jnp.dot(
        turned,
        swapped[:, model_width // blocks : body_width].reshape(blocks, -1),
        preferred_element_type=jnp.float32,
    ).reshape(blocks * own_rows, -1)
    part = jnp.dot(features, mixer_weight, preferred_element_type=jnp.float32).astype(jnp.bfloat16)
    projected = added_on_arrival(part.reshape(blocks, own_rows, -1), "ep", far)
    first_expert = lax.axis_index("ep") // NEAR * NEAR
    experts = (first_expert + jnp.arange(NEAR)).astype(jnp.float32)
    hits = tail_in[:, :top_count, None] == experts[None, None, :]
    picked = slots_of(jnp.any(hits, axis=1), own_rows, capacity)
    dispatch = picked.reshape(-1, blocks * own_rows).astype(jnp.bfloat16)

    def shares_by_slot(first):
        by_expert = jnp.sum(jnp.where(hits, tail_in[:, first : first + top_count, None], 0.0), axis=1)
        spread = jnp.where(picked, by_expert.T[:, None, :], 0.0)
        return spread.reshape(-1, blocks * own_rows).astype(jnp.bfloat16)

    gather_high, gather_low = shares_by_slot(top_count), shares_by_slot(2 * top_count)
    decay_rate, learn_rate, gating = channel_rates(
        tokens,
        decay_lowrank_first,
        decay_lowrank_second,
        decay_channel_offset,
        correction_lowrank_first,
        correction_lowrank_second,
        correction_offset,
        gate_lowrank_first,
        gate_lowrank_second,
    )
    mixer_result, next_state = recurrence(
        projected,
        decay_rate,
        learn_rate,
        gating,
        key_rate_blend,
        self_token_scale,
        per_head_gain,
        per_head_bias,
        prior_state,
    )
    by_holder = mixer_result.reshape(own_rows, blocks, NEAR, -1).swapaxes(1, 2)
    channels = lax.all_to_all(
        by_holder.reshape(own_rows, NEAR, -1),
        "ep", split_axis=1, concat_axis=0, tiled=True, axis_index_groups=near,
    ).reshape(NEAR * own_rows, -1)
    mixed_part = jnp.dot(channels, output_weight, preferred_element_type=jnp.float32)
    mixed = added_on_arrival(
        mixed_part.astype(jnp.bfloat16).reshape(NEAR, own_rows, model_width), "ep", near
    )
    hidden = layer_norm(
        tokens.astype(jnp.float32) + mixed, mixer_norm_gain, mixer_norm_bias
    ).astype(jnp.bfloat16)
    class_rows = jnp.concatenate([hidden] + [shifted(hidden, "ep", k) for k in range(1, blocks)])
    outgoing = jnp.dot(dispatch, class_rows, preferred_element_type=jnp.float32).astype(jnp.bfloat16)
    arrived = lax.all_to_all(
        outgoing.reshape(NEAR, -1, model_width), "ep", 0, 0, tiled=True, axis_index_groups=near
    )
    flat_in = arrived.reshape(-1, model_width)
    gate_val = jnp.dot(flat_in, expert_gate_weight[0], preferred_element_type=jnp.float32)
    up_val = jnp.dot(flat_in, expert_up_weight[0], preferred_element_type=jnp.float32)
    inner = (jax.nn.silu(gate_val) * up_val).astype(jnp.bfloat16)
    produced = jnp.dot(inner, expert_down_weight[0], preferred_element_type=jnp.float32).astype(
        jnp.bfloat16
    )
    returned = lax.all_to_all(
        produced.reshape(NEAR, -1, model_width), "ep", 0, 0, tiled=True, axis_index_groups=near
    ).reshape(-1, model_width)
    over_slots = (((0,), (0,)), ((), ()))
    block_sum = lax.dot_general(
        gather_high, returned, over_slots, preferred_element_type=jnp.float32
    ) + lax.dot_general(gather_low, returned, over_slots, preferred_element_type=jnp.float32)
    block_sum = block_sum.astype(jnp.bfloat16).reshape(blocks, own_rows, model_width)
    combined = block_sum[0].astype(jnp.float32)
    for k in range(1, blocks):
        combined = combined + shifted(block_sum[k], "ep", -k).astype(jnp.float32)
    result = layer_norm(
        hidden.astype(jnp.float32) + combined, expert_norm_gain, expert_norm_bias
    ).astype(jnp.bfloat16)
    return (result, next_state)


def solution(mesh):
    in_specs = (
        P(("grp", "ep"), None),
        P(("grp", "ep"), None, None, None),
        P("ep", None),
        P("ep", None),
        P("ep", None),
        P(),
        P(),
        P(),
        P(),
        P(),
        P(),
        P(),
        P(),
        P(),
        P(),
        P(),
        P(),
        P("ep", None),
        P(),
        P(),
        P(),
        P(),
        P(("grp", "ep"), None),
        P(("grp", "ep"), None),
        P("ep", None, None),
        P("ep", None, None),
        P("ep", None, None),
    )
    out_specs = (P(("grp", "ep"), None), P(("grp", "ep"), None, None, None))
    return jax.shard_map(body, mesh=mesh, in_specs=in_specs, out_specs=out_specs, check_vma=False)
```

```python
import jax
import jax.numpy as jnp
from jax import lax
from jax.experimental import pallas as pl
from jax.sharding import PartitionSpec as P


NEAR = 8
GROUP = 8


def near_and_far(axis):
    devices = lax.axis_size(axis)
    blocks = devices // NEAR
    near = [[NEAR * b + j for j in range(NEAR)] for b in range(blocks)]
    far = [[NEAR * b + j for b in range(blocks)] for j in range(NEAR)]
    return near, far


def added_on_arrival(parts, axis, groups):
    got = lax.all_to_all(parts, axis, split_axis=0, concat_axis=0, tiled=True, axis_index_groups=groups)
    return jnp.sum(got.astype(jnp.float32), axis=0)


def slots_of(named, own_rows, capacity):
    owners = named.shape[0] // own_rows
    marks = named.reshape(owners, own_rows, -1).astype(jnp.float32)
    earlier = jnp.einsum("pr,orn->opn", jnp.tri(own_rows, k=-1, dtype=jnp.float32), marks)
    place = jnp.arange(owners, dtype=jnp.float32)[:, None, None] * capacity + earlier
    place = jnp.where(marks > 0, place, -1.0).reshape(owners * own_rows, -1)
    slots = jnp.arange(owners * capacity, dtype=jnp.float32)
    return place.T[:, None, :] == slots[None, :, None]


def layer_norm(values_in, gain_vec, bias_vec):
    row_mean = jnp.mean(values_in, -1, keepdims=True)
    centered = values_in - row_mean
    row_var = jnp.mean(centered * centered, -1, keepdims=True)
    return centered * lax.rsqrt(row_var + 1e-05) * gain_vec + bias_vec


def recurrence_step(projected_ref, decay_ref, learn_ref, gating_ref, blend_ref, own_ref, gain_ref, bias_ref,
                    state_ref, mixer_ref, next_ref):
    heads, size = decay_ref.shape[1], decay_ref.shape[2]
    receptance = projected_ref[0, 0:heads]
    key = projected_ref[0, heads : 2 * heads]
    value = projected_ref[0, 2 * heads : 3 * heads]
    decay, learn = decay_ref[0], learn_ref[0]
    unit = key * lax.rsqrt(jnp.sum(key * key, -1, keepdims=True) + 1e-06)
    written = key * (1.0 + (learn - 1.0) * blend_ref[...])
    unit_learn = unit * learn
    decayed = decay * receptance
    value_columns = value.T
    lane = lax.broadcasted_iota(jnp.int32, (size, heads), 1)
    removed_columns = jnp.zeros((size, heads), jnp.float32)
    kept_columns = jnp.zeros((size, heads), jnp.float32)

    def sums(h):
        state, at = state_ref[0, h], slice(h, h + 1)
        return (
            jnp.sum(state * unit[at], -1, keepdims=True),
            jnp.sum(state * decayed[at], -1, keepdims=True),
        )

    for first in range(0, heads, GROUP):
        held = [sums(h) for h in range(first, first + GROUP)]
        for h, (removed, kept) in zip(range(first, first + GROUP), held):
            at = slice(h, h + 1)
            next_ref[0, h] = (
                state_ref[0, h] * decay[at]
                - removed * unit_learn[at]
                + value_columns[:, at] * written[at]
            )
            removed_columns = jnp.where(lane == h, removed, removed_columns)
            kept_columns = jnp.where(lane == h, kept, kept_columns)
    readout = (
        kept_columns.T
        - removed_columns.T * jnp.sum(unit_learn * receptance, -1, keepdims=True)
        + value * jnp.sum(written * receptance, -1, keepdims=True)
    )
    centered = readout - jnp.mean(readout, -1, keepdims=True)
    spread = jnp.mean(centered * centered, -1, keepdims=True)
    normed = centered * lax.rsqrt(spread + 0.00064) * gain_ref[...] + bias_ref[...]
    own = jnp.sum(receptance * written * own_ref[...], -1, keepdims=True) * value
    mixer_ref[0] = ((normed + own) * gating_ref[0]).astype(jnp.bfloat16)


def recurrence(projected, decay, learn, gating, blend, own, gain, bias, state, interpret=False):
    rows, heads, size = state.shape[:3]
    by_row = pl.BlockSpec((1, heads, size), lambda t: (t, 0, 0))
    by_channel = pl.BlockSpec((heads, size), lambda t: (0, 0))
    by_state = pl.BlockSpec((1, heads, size, size), lambda t: (t, 0, 0, 0))

    def cut(flat):
        return flat.reshape(*flat.shape[:-1], -1, size)

    return pl.pallas_call(
        recurrence_step,
        grid=(rows,),
        in_specs=[pl.BlockSpec((1, 3 * heads, size), lambda t: (t, 0, 0))]
        + [by_row] * 3 + [by_channel] * 4 + [by_state],
        out_specs=[by_row, by_state],
        out_shape=[
            jax.ShapeDtypeStruct((rows, heads, size), jnp.bfloat16),
            jax.ShapeDtypeStruct(state.shape, jnp.float32),
        ],
        name="recurrence",
        interpret=interpret,
    )(cut(projected), cut(decay), cut(learn), cut(gating), cut(blend), own, cut(gain), cut(bias), state)


def channel_rates(
    tokens,
    decay_lowrank_first,
    decay_lowrank_second,
    decay_channel_offset,
    correction_lowrank_first,
    correction_lowrank_second,
    correction_offset,
    gate_lowrank_first,
    gate_lowrank_second,
):
    squash = jnp.tanh(
        jnp.dot(tokens, decay_lowrank_first, preferred_element_type=jnp.float32)
    ).astype(jnp.bfloat16)
    pre_decay = decay_channel_offset + jnp.dot(
        squash, decay_lowrank_second, preferred_element_type=jnp.float32
    )
    decay_rate = jnp.exp(-jnp.exp(-jax.nn.softplus(-pre_decay) - 0.5))
    low_learn = jnp.dot(
        tokens, correction_lowrank_first, preferred_element_type=jnp.float32
    ).astype(jnp.bfloat16)
    learn_rate = jax.nn.sigmoid(
        correction_offset
        + jnp.dot(low_learn, correction_lowrank_second, preferred_element_type=jnp.float32)
    )
    opened = jax.nn.sigmoid(
        jnp.dot(tokens, gate_lowrank_first, preferred_element_type=jnp.float32)
    ).astype(jnp.bfloat16)
    gating = jnp.dot(opened, gate_lowrank_second, preferred_element_type=jnp.float32)
    return decay_rate, learn_rate, gating


def body(
    tokens,
    prior_state,
    receptance_matrix,
    key_matrix,
    value_matrix,
    decay_lowrank_first,
    decay_lowrank_second,
    decay_channel_offset,
    correction_lowrank_first,
    correction_lowrank_second,
    correction_offset,
    gate_lowrank_first,
    gate_lowrank_second,
    key_rate_blend,
    self_token_scale,
    per_head_gain,
    per_head_bias,
    mixer_output_weight,
    mixer_norm_gain,
    mixer_norm_bias,
    expert_norm_gain,
    expert_norm_bias,
    routes,
    routing_weight,
    expert_gate_weight,
    expert_up_weight,
    expert_down_weight,
):
    own_rows, model_width = tokens.shape
    top_count = routes.shape[1]
    near, far = near_and_far("ep")
    blocks = len(near)
    expert_count = lax.axis_size("ep")
    capacity = max(2, 2 * own_rows * top_count // expert_count)
    mixer_weight = lax.all_gather(
        jnp.concatenate((receptance_matrix, key_matrix, value_matrix), axis=1),
        "ep", axis=0, tiled=True, axis_index_groups=near,
    )
    groups = lax.axis_size("grp")
    share_rows = mixer_output_weight.shape[0] // groups
    weight_share = lax.dynamic_slice_in_dim(
        mixer_output_weight, lax.axis_index("grp") * share_rows, share_rows
    ).reshape(own_rows, 1, -1)
    share = routing_weight / jnp.sum(routing_weight, -1, keepdims=True)
    share_high = lax.reduce_precision(share, 8, 7)
    tail = jnp.concatenate((routes.astype(jnp.float32), share_high, share - share_high), axis=1)
    tail = jnp.pad(tail.astype(jnp.bfloat16), ((0, 0), (0, 128 - tail.shape[1])))
    sent = jnp.concatenate(
        (
            tokens.reshape(own_rows, blocks, -1),
            jnp.broadcast_to(weight_share, (own_rows, blocks, weight_share.shape[2])),
        ),
        axis=2,
    )
    swapped = lax.all_to_all(sent, "ep", split_axis=1, concat_axis=0, tiled=True, axis_index_groups=far)
    swapped = swapped.reshape(blocks * own_rows, -1)
    body_width = model_width // blocks
    output_weight = lax.all_gather(
        swapped[:, body_width:].reshape(blocks, share_rows, model_width), "grp", axis=1, tiled=True
    ).reshape(-1, model_width)
    features = swapped[:, :body_width]
    part = jnp.dot(features, mixer_weight, preferred_element_type=jnp.float32).astype(jnp.bfloat16)
    part = jnp.concatenate(
        (
            part.reshape(blocks, own_rows, -1),
            jnp.broadcast_to(tail[None], (blocks, own_rows, tail.shape[1])),
        ),
        axis=2,
    )
    arrived_parts = lax.all_to_all(part, "ep", 0, 0, tiled=True, axis_index_groups=far)
    mixer_width = mixer_weight.shape[1]
    projected = jnp.sum(arrived_parts[:, :, :mixer_width].astype(jnp.float32), axis=0)
    tail_in = arrived_parts[:, :, mixer_width:].astype(jnp.float32).reshape(blocks * own_rows, -1)
    first_expert = lax.axis_index("ep") // NEAR * NEAR
    experts = (first_expert + jnp.arange(NEAR)).astype(jnp.float32)
    hits = tail_in[:, :top_count, None] == experts[None, None, :]
    picked = slots_of(jnp.any(hits, axis=1), own_rows, capacity)
    dispatch = picked.reshape(-1, blocks * own_rows).astype(jnp.bfloat16)

    def shares_by_slot(first):
        by_expert = jnp.sum(jnp.where(hits, tail_in[:, first : first + top_count, None], 0.0), axis=1)
        spread = jnp.where(picked, by_expert.T[:, None, :], 0.0)
        return spread.reshape(-1, blocks * own_rows).astype(jnp.bfloat16)

    gather_high, gather_low = shares_by_slot(top_count), shares_by_slot(2 * top_count)
    decay_rate, learn_rate, gating = channel_rates(
        tokens,
        decay_lowrank_first,
        decay_lowrank_second,
        decay_channel_offset,
        correction_lowrank_first,
        correction_lowrank_second,
        correction_offset,
        gate_lowrank_first,
        gate_lowrank_second,
    )
    mixer_result, next_state = recurrence(
        projected,
        decay_rate,
        learn_rate,
        gating,
        key_rate_blend,
        self_token_scale,
        per_head_gain,
        per_head_bias,
        prior_state,
    )
    by_holder = mixer_result.reshape(own_rows, blocks, NEAR, -1).swapaxes(1, 2)
    channels = lax.all_to_all(
        by_holder.reshape(own_rows, NEAR, -1),
        "ep", split_axis=1, concat_axis=0, tiled=True, axis_index_groups=near,
    ).reshape(NEAR * own_rows, -1)
    mixed_part = jnp.dot(channels, output_weight, preferred_element_type=jnp.float32)
    mixed = added_on_arrival(
        mixed_part.astype(jnp.bfloat16).reshape(NEAR, own_rows, model_width), "ep", near
    )
    hidden = layer_norm(
        tokens.astype(jnp.float32) + mixed, mixer_norm_gain, mixer_norm_bias
    ).astype(jnp.bfloat16)
    class_rows = lax.all_to_all(
        jnp.broadcast_to(hidden[None], (blocks, own_rows, model_width)),
        "ep", 0, 0, tiled=True, axis_index_groups=far,
    ).reshape(blocks * own_rows, model_width)
    outgoing = jnp.dot(dispatch, class_rows, preferred_element_type=jnp.float32).astype(jnp.bfloat16)
    arrived = lax.all_to_all(
        outgoing.reshape(NEAR, -1, model_width), "ep", 0, 0, tiled=True, axis_index_groups=near
    )
    flat_in = arrived.reshape(-1, model_width)
    gate_val = jnp.dot(flat_in, expert_gate_weight[0], preferred_element_type=jnp.float32)
    up_val = jnp.dot(flat_in, expert_up_weight[0], preferred_element_type=jnp.float32)
    inner = (jax.nn.silu(gate_val) * up_val).astype(jnp.bfloat16)
    produced = jnp.dot(inner, expert_down_weight[0], preferred_element_type=jnp.float32).astype(
        jnp.bfloat16
    )
    returned = lax.all_to_all(
        produced.reshape(NEAR, -1, model_width), "ep", 0, 0, tiled=True, axis_index_groups=near
    ).reshape(-1, model_width)
    over_slots = (((0,), (0,)), ((), ()))
    block_sum = lax.dot_general(
        gather_high, returned, over_slots, preferred_element_type=jnp.float32
    ) + lax.dot_general(gather_low, returned, over_slots, preferred_element_type=jnp.float32)
    combined = added_on_arrival(
        block_sum.astype(jnp.bfloat16).reshape(blocks, own_rows, model_width), "ep", far
    )
    result = layer_norm(
        hidden.astype(jnp.float32) + combined, expert_norm_gain, expert_norm_bias
    ).astype(jnp.bfloat16)
    return (result, next_state)


def solution(mesh):
    in_specs = (
        P(("grp", "ep"), None),
        P(("grp", "ep"), None, None, None),
        P("ep", None),
        P("ep", None),
        P("ep", None),
        P(),
        P(),
        P(),
        P(),
        P(),
        P(),
        P(),
        P(),
        P(),
        P(),
        P(),
        P(),
        P("ep", None),
        P(),
        P(),
        P(),
        P(),
        P(("grp", "ep"), None),
        P(("grp", "ep"), None),
        P("ep", None, None),
        P("ep", None, None),
        P("ep", None, None),
    )
    out_specs = (P(("grp", "ep"), None), P(("grp", "ep"), None, None, None))
    return jax.shard_map(body, mesh=mesh, in_specs=in_specs, out_specs=out_specs, check_vma=False)
```

```python
import jax
import jax.numpy as jnp
from jax import lax
from jax.experimental import pallas as pl
from jax.sharding import PartitionSpec as P


NEAR = 8
GROUP = 16


def near_and_far(axis):
    devices = lax.axis_size(axis)
    blocks = devices // NEAR
    near = [[NEAR * b + j for j in range(NEAR)] for b in range(blocks)]
    far = [[NEAR * b + j for b in range(blocks)] for j in range(NEAR)]
    return near, far


def added_on_arrival(parts, axis, groups):
    got = lax.all_to_all(parts, axis, split_axis=0, concat_axis=0, tiled=True, axis_index_groups=groups)
    return jnp.sum(got.astype(jnp.float32), axis=0)


def slots_of(named, own_rows, capacity):
    owners = named.shape[0] // own_rows
    marks = named.reshape(owners, own_rows, -1).astype(jnp.float32)
    earlier = jnp.einsum("pr,orn->opn", jnp.tri(own_rows, k=-1, dtype=jnp.float32), marks)
    place = jnp.arange(owners, dtype=jnp.float32)[:, None, None] * capacity + earlier
    place = jnp.where(marks > 0, place, -1.0).reshape(owners * own_rows, -1)
    slots = jnp.arange(owners * capacity, dtype=jnp.float32)
    return place.T[:, None, :] == slots[None, :, None]


def layer_norm(values_in, gain_vec, bias_vec):
    row_mean = jnp.mean(values_in, -1, keepdims=True)
    centered = values_in - row_mean
    row_var = jnp.mean(centered * centered, -1, keepdims=True)
    return centered * lax.rsqrt(row_var + 1e-05) * gain_vec + bias_vec


def recurrence_step(projected_ref, rates_ref, fixed_ref, state_ref, mixer_ref, next_ref):
    heads, size = mixer_ref.shape[1], mixer_ref.shape[2]
    receptance, key, value = (projected_ref[0, k * heads : (k + 1) * heads] for k in range(3))
    decay, learn, gating = (rates_ref[0, k * heads : (k + 1) * heads] for k in range(3))
    blend, own_scale, gain, bias = (fixed_ref[k * heads : (k + 1) * heads] for k in range(4))
    unit = key * lax.rsqrt(jnp.sum(key * key, -1, keepdims=True) + 1e-06)
    written = key * (1.0 + (learn - 1.0) * blend)
    unit_learn = unit * learn
    decayed = decay * receptance
    value_columns = value.T
    lane = lax.broadcasted_iota(jnp.int32, (size, heads), 1)
    removed_columns = jnp.zeros((size, heads), jnp.float32)
    kept_columns = jnp.zeros((size, heads), jnp.float32)

    def sums(h):
        state, at = state_ref[0, h], slice(h, h + 1)
        return (
            jnp.sum(state * unit[at], -1, keepdims=True),
            jnp.sum(state * decayed[at], -1, keepdims=True),
        )

    for first in range(0, heads, GROUP):
        held = [sums(h) for h in range(first, first + GROUP)]
        for h, (removed, kept) in zip(range(first, first + GROUP), held):
            at = slice(h, h + 1)
            next_ref[0, h] = (
                state_ref[0, h] * decay[at]
                - removed * unit_learn[at]
                + value_columns[:, at] * written[at]
            )
            removed_columns = jnp.where(lane == h, removed, removed_columns)
            kept_columns = jnp.where(lane == h, kept, kept_columns)
    readout = (
        kept_columns.T
        - removed_columns.T * jnp.sum(unit_learn * receptance, -1, keepdims=True)
        + value * jnp.sum(written * receptance, -1, keepdims=True)
    )
    centered = readout - jnp.mean(readout, -1, keepdims=True)
    spread = jnp.mean(centered * centered, -1, keepdims=True)
    normed = centered * lax.rsqrt(spread + 0.00064) * gain + bias
    own = jnp.sum(receptance * written * own_scale, -1, keepdims=True) * value
    mixer_ref[0] = ((normed + own) * gating).astype(jnp.bfloat16)


def recurrence(projected, decay, learn, gating, blend, own, gain, bias, state):
    rows, heads, size = state.shape[:3]
    by_row = pl.BlockSpec((1, 3 * heads, size), lambda t: (t, 0, 0))
    by_state = pl.BlockSpec((1, heads, size, size), lambda t: (t, 0, 0, 0))
    rates = jnp.concatenate((decay, learn, gating), axis=1).reshape(rows, -1, size)
    fixed = jnp.concatenate((blend, own.reshape(-1), gain, bias)).reshape(-1, size)
    return pl.pallas_call(
        recurrence_step,
        grid=(rows,),
        in_specs=[
            by_row,
            by_row,
            pl.BlockSpec((4 * heads, size), lambda t: (0, 0)),
            by_state,
        ],
        out_specs=[pl.BlockSpec((1, heads, size), lambda t: (t, 0, 0)), by_state],
        out_shape=[
            jax.ShapeDtypeStruct((rows, heads, size), jnp.bfloat16),
            jax.ShapeDtypeStruct(state.shape, jnp.float32),
        ],
        name="recurrence",
    )(projected.reshape(rows, -1, size), rates, fixed, state)


def channel_rates(
    tokens,
    decay_lowrank_first,
    decay_lowrank_second,
    decay_channel_offset,
    correction_lowrank_first,
    correction_lowrank_second,
    correction_offset,
    gate_lowrank_first,
    gate_lowrank_second,
):
    squash = jnp.tanh(
        jnp.dot(tokens, decay_lowrank_first, preferred_element_type=jnp.float32)
    ).astype(jnp.bfloat16)
    pre_decay = decay_channel_offset + jnp.dot(
        squash, decay_lowrank_second, preferred_element_type=jnp.float32
    )
    decay_rate = jnp.exp(-jnp.exp(-jax.nn.softplus(-pre_decay) - 0.5))
    low_learn = jnp.dot(
        tokens, correction_lowrank_first, preferred_element_type=jnp.float32
    ).astype(jnp.bfloat16)
    learn_rate = jax.nn.sigmoid(
        correction_offset
        + jnp.dot(low_learn, correction_lowrank_second, preferred_element_type=jnp.float32)
    )
    opened = jax.nn.sigmoid(
        jnp.dot(tokens, gate_lowrank_first, preferred_element_type=jnp.float32)
    ).astype(jnp.bfloat16)
    gating = jnp.dot(opened, gate_lowrank_second, preferred_element_type=jnp.float32)
    return decay_rate, learn_rate, gating


def body(
    tokens,
    prior_state,
    receptance_matrix,
    key_matrix,
    value_matrix,
    decay_lowrank_first,
    decay_lowrank_second,
    decay_channel_offset,
    correction_lowrank_first,
    correction_lowrank_second,
    correction_offset,
    gate_lowrank_first,
    gate_lowrank_second,
    key_rate_blend,
    self_token_scale,
    per_head_gain,
    per_head_bias,
    mixer_output_weight,
    mixer_norm_gain,
    mixer_norm_bias,
    expert_norm_gain,
    expert_norm_bias,
    routes,
    routing_weight,
    expert_gate_weight,
    expert_up_weight,
    expert_down_weight,
):
    own_rows, model_width = tokens.shape
    top_count = routes.shape[1]
    near, far = near_and_far("ep")
    blocks = len(near)
    expert_count = lax.axis_size("ep")
    capacity = max(2, 2 * own_rows * top_count // expert_count)
    mixer_weight = lax.all_gather(
        jnp.concatenate((receptance_matrix, key_matrix, value_matrix), axis=1),
        "ep", axis=0, tiled=True, axis_index_groups=near,
    )
    groups = lax.axis_size("grp")
    share_rows = mixer_output_weight.shape[0] // groups
    weight_share = lax.dynamic_slice_in_dim(
        mixer_output_weight, lax.axis_index("grp") * share_rows, share_rows
    ).reshape(own_rows, 1, -1)
    share = routing_weight / jnp.sum(routing_weight, -1, keepdims=True)
    share_high = lax.reduce_precision(share, 8, 7)
    tail = jnp.concatenate((routes.astype(jnp.float32), share_high, share - share_high), axis=1)
    tail = jnp.pad(tail.astype(jnp.bfloat16), ((0, 0), (0, 128 - tail.shape[1])))
    sent = jnp.concatenate(
        (
            tokens.reshape(own_rows, blocks, -1),
            jnp.broadcast_to(weight_share, (own_rows, blocks, weight_share.shape[2])),
        ),
        axis=2,
    )
    swapped = lax.all_to_all(sent, "ep", split_axis=1, concat_axis=0, tiled=True, axis_index_groups=far)
    swapped = swapped.reshape(blocks * own_rows, -1)
    body_width = model_width // blocks
    output_weight = lax.all_gather(
        swapped[:, body_width:].reshape(blocks, share_rows, model_width), "grp", axis=1, tiled=True
    ).reshape(-1, model_width)
    features = swapped[:, :body_width]
    part = jnp.dot(features, mixer_weight, preferred_element_type=jnp.float32).astype(jnp.bfloat16)
    part = jnp.concatenate(
        (
            part.reshape(blocks, own_rows, -1),
            jnp.broadcast_to(tail[None], (blocks, own_rows, tail.shape[1])),
        ),
        axis=2,
    )
    arrived_parts = lax.all_to_all(part, "ep", 0, 0, tiled=True, axis_index_groups=far)
    mixer_width = mixer_weight.shape[1]
    projected = jnp.sum(arrived_parts[:, :, :mixer_width].astype(jnp.float32), axis=0)
    tail_in = arrived_parts[:, :, mixer_width:].astype(jnp.float32).reshape(blocks * own_rows, -1)
    first_expert = lax.axis_index("ep") // NEAR * NEAR
    experts = (first_expert + jnp.arange(NEAR)).astype(jnp.float32)
    hits = tail_in[:, :top_count, None] == experts[None, None, :]
    picked = slots_of(jnp.any(hits, axis=1), own_rows, capacity)
    dispatch = picked.reshape(-1, blocks * own_rows).astype(jnp.bfloat16)

    def shares_by_slot(first):
        by_expert = jnp.sum(jnp.where(hits, tail_in[:, first : first + top_count, None], 0.0), axis=1)
        spread = jnp.where(picked, by_expert.T[:, None, :], 0.0)
        return spread.reshape(-1, blocks * own_rows).astype(jnp.bfloat16)

    gather_high, gather_low = shares_by_slot(top_count), shares_by_slot(2 * top_count)
    decay_rate, learn_rate, gating = channel_rates(
        tokens,
        decay_lowrank_first,
        decay_lowrank_second,
        decay_channel_offset,
        correction_lowrank_first,
        correction_lowrank_second,
        correction_offset,
        gate_lowrank_first,
        gate_lowrank_second,
    )
    mixer_result, next_state = recurrence(
        projected,
        decay_rate,
        learn_rate,
        gating,
        key_rate_blend,
        self_token_scale,
        per_head_gain,
        per_head_bias,
        prior_state,
    )
    by_holder = mixer_result.reshape(own_rows, blocks, NEAR, -1).swapaxes(1, 2)
    channels = lax.all_to_all(
        by_holder.reshape(own_rows, NEAR, -1),
        "ep", split_axis=1, concat_axis=0, tiled=True, axis_index_groups=near,
    ).reshape(NEAR * own_rows, -1)
    mixed_part = jnp.dot(channels, output_weight, preferred_element_type=jnp.float32)
    mixed = added_on_arrival(
        mixed_part.astype(jnp.bfloat16).reshape(NEAR, own_rows, model_width), "ep", near
    )
    hidden = layer_norm(
        tokens.astype(jnp.float32) + mixed, mixer_norm_gain, mixer_norm_bias
    ).astype(jnp.bfloat16)
    class_rows = lax.all_to_all(
        jnp.broadcast_to(hidden[None], (blocks, own_rows, model_width)),
        "ep", 0, 0, tiled=True, axis_index_groups=far,
    ).reshape(blocks * own_rows, model_width)
    outgoing = jnp.dot(dispatch, class_rows, preferred_element_type=jnp.float32).astype(jnp.bfloat16)
    arrived = lax.all_to_all(
        outgoing.reshape(NEAR, -1, model_width), "ep", 0, 0, tiled=True, axis_index_groups=near
    )
    flat_in = arrived.reshape(-1, model_width)
    gate_val = jnp.dot(flat_in, expert_gate_weight[0], preferred_element_type=jnp.float32)
    up_val = jnp.dot(flat_in, expert_up_weight[0], preferred_element_type=jnp.float32)
    inner = (jax.nn.silu(gate_val) * up_val).astype(jnp.bfloat16)
    produced = jnp.dot(inner, expert_down_weight[0], preferred_element_type=jnp.float32).astype(
        jnp.bfloat16
    )
    returned = lax.all_to_all(
        produced.reshape(NEAR, -1, model_width), "ep", 0, 0, tiled=True, axis_index_groups=near
    ).reshape(-1, model_width)
    over_slots = (((0,), (0,)), ((), ()))
    block_sum = lax.dot_general(
        gather_high, returned, over_slots, preferred_element_type=jnp.float32
    ) + lax.dot_general(gather_low, returned, over_slots, preferred_element_type=jnp.float32)
    combined = added_on_arrival(
        block_sum.astype(jnp.bfloat16).reshape(blocks, own_rows, model_width), "ep", far
    )
    result = layer_norm(
        hidden.astype(jnp.float32) + combined, expert_norm_gain, expert_norm_bias
    ).astype(jnp.bfloat16)
    return (result, next_state)


def solution(mesh):
    in_specs = (
        P(("grp", "ep"), None),
        P(("grp", "ep"), None, None, None),
        P("ep", None),
        P("ep", None),
        P("ep", None),
        P(),
        P(),
        P(),
        P(),
        P(),
        P(),
        P(),
        P(),
        P(),
        P(),
        P(),
        P(),
        P("ep", None),
        P(),
        P(),
        P(),
        P(),
        P(("grp", "ep"), None),
        P(("grp", "ep"), None),
        P("ep", None, None),
        P("ep", None, None),
        P("ep", None, None),
    )
    out_specs = (P(("grp", "ep"), None), P(("grp", "ep"), None, None, None))
    return jax.shard_map(body, mesh=mesh, in_specs=in_specs, out_specs=out_specs, check_vma=False)
```
